32 devices in a mesh: sp: 4 (over z), tp: 8 (over y, x, core).
Axes of the slice: x: 2, y: 2, z: 4, core: 2. Of those that a mesh axis runs over, the one named last changes fastest.
Arguments:
- target_rows: bfloat16 [768, 2048], P(('sp', 'tp')), may hold values from -6 to 6
- source_rows: bfloat16 [4096, 2048], P(('sp', 'tp')), may hold values from -6 to 6
- target_gain: float32 [2048], replicated, may hold values from 0.55 to 9
- source_gain: float32 [2048], replicated, may hold values from 0.55 to 9
- query_weight: bfloat16 [2048, 2048], P(None, 'tp'), may hold values from -0.125 to 0.125
- key_weight: bfloat16 [2048, 512], P('tp'), may hold values from -0.125 to 0.125
- value_weight: bfloat16 [2048, 512], P('tp'), may hold values from -0.125 to 0.125
- out_weight: bfloat16 [2048, 2048], P('tp'), may hold values from -0.125 to 0.125
- out_cotangent: bfloat16 [768, 2048], P(('sp', 'tp')), may hold values from -6 to 6
Outputs:
- target_grad: float32 [768, 2048], P(('sp', 'tp'))
- source_grad: float32 [4096, 2048], P(('sp', 'tp'))
- out_weight_grad: float32 [2048, 2048], P('tp')
The draws below stay inside these ranges and needn't reach their ends.
All inputs are finite; a program needn't handle non-finite values.
Results may differ from the reference program's by a relative error of at most 0.03.
Values may be sent and summed in bfloat16 or wider, within the bound.
No kernel may reach another device: no remote copies, remote signals or barrier semaphores. Data moves between devices by JAX's collectives and lax.ppermute only.
A program may use at most 64 MiB of HBM per device.

```python
import jax
import jax.numpy as jnp
from jax import lax

D = 2048
HEADS = 32
HEAD_DIM = 64
KV_HEADS = 8
TGT_ALL = 768
SRC_ALL = 4096


def gain_draw(seed_key):
    return 1.0 + 0.18 * jax.random.truncated_normal(seed_key, -2.5, 2.5, (D,), jnp.float32)


def draw_target_gain(key, part):
    return gain_draw(jax.random.fold_in(key, 11))


def draw_source_gain(key, part):
    return gain_draw(jax.random.fold_in(key, 23))


def steps_of(key, extent, cuts, least, largest):
    level = 1.0
    for axis_at, blocks in cuts:
        heights = jax.random.uniform(jax.random.fold_in(jax.random.fold_in(key, 6), axis_at), (blocks,), jnp.float32, least / len(cuts), largest / len(cuts))
        level = level * jnp.repeat(jnp.exp(heights), extent[axis_at] // blocks).reshape((-1,) + (1,) * (len(extent) - 1 - axis_at))
    return level


def scatter_about(key, extent, spread, bound, shards=(), kind=jnp.bfloat16):
    drawn = jax.random.normal(key, extent, jnp.float32) * spread
    if len(shards) > 0:
        drawn = steps_of(key, extent, shards, -0.22, 0.18) * drawn
    return jnp.clip(drawn, min=-bound, max=bound).astype(kind)


def setup_inputs(seed: int = 0) -> dict:
    streams_of = jax.random.split(jax.random.key(seed), 10)
    return {
        "target_rows": scatter_about(streams_of[0], (TGT_ALL, D), 1.0, 6.0, ((0, 32),)),
        "source_rows": scatter_about(streams_of[1], (SRC_ALL, D), 1.0, 6.0, ((0, 32),)),
        "target_gain": draw_target_gain(jax.random.fold_in(streams_of[9], 71), 0),
        "source_gain": draw_source_gain(jax.random.fold_in(streams_of[9], 71), 0),
        "query_weight": scatter_about(streams_of[4], (D, HEADS * HEAD_DIM), D ** -0.5, 0.125, ((1, 8),)),
        "key_weight": scatter_about(streams_of[5], (D, KV_HEADS * HEAD_DIM), D ** -0.5, 0.125, ((0, 8),)),
        "value_weight": scatter_about(streams_of[6], (D, KV_HEADS * HEAD_DIM), D ** -0.5, 0.125, ((0, 8),)),
        "out_weight": scatter_about(streams_of[7], (HEADS * HEAD_DIM, D), (HEADS * HEAD_DIM) ** -0.5, 0.125, ((0, 8),)),
        "out_cotangent": scatter_about(streams_of[8], (TGT_ALL, D), 1.0, 6.0, ((0, 32),)),
    }


EPSILON = 1e-06

def normalize(matrix, gain_vector):
    widened = matrix.astype(jnp.float32)
    factor = lax.rsqrt(lax.optimization_barrier(jnp.mean(widened * widened, axis=-1, keepdims=True)) + EPSILON)
    return (widened * factor * gain_vector).astype(jnp.bfloat16)

def norm_back(matrix, gain_vector, upstream):
    widened = matrix.astype(jnp.float32)
    factor = lax.rsqrt(lax.optimization_barrier(jnp.mean(widened * widened, axis=-1, keepdims=True)) + EPSILON)
    weighted = upstream * gain_vector
    inner_sum = lax.optimization_barrier(jnp.mean(weighted * widened, axis=-1, keepdims=True))
    return factor * weighted - widened * factor ** 3 * inner_sum

def reference(target_rows, source_rows, target_gain, source_gain, query_weight, key_weight, value_weight, out_weight, out_cotangent):
    score_scale = HEAD_DIM ** (-0.5)
    group_size = HEADS // KV_HEADS
    normed_t = normalize(target_rows, target_gain)
    normed_s = normalize(source_rows, source_gain)
    queries = jnp.dot(normed_t, query_weight, preferred_element_type=jnp.float32).astype(jnp.bfloat16)
    keys_all = jnp.dot(normed_s, key_weight, preferred_element_type=jnp.float32).astype(jnp.bfloat16)
    values_all = jnp.dot(normed_s, value_weight, preferred_element_type=jnp.float32).astype(jnp.bfloat16)
    query_heads = queries.reshape(TGT_ALL, HEADS, HEAD_DIM).transpose(1, 0, 2)
    key_heads = keys_all.reshape(SRC_ALL, KV_HEADS, HEAD_DIM).transpose(1, 0, 2)
    value_heads = values_all.reshape(SRC_ALL, KV_HEADS, HEAD_DIM).transpose(1, 0, 2)
    out_heads = out_weight.reshape(HEADS, HEAD_DIM, D)

    def one_head(head_index):
        query = query_heads[head_index]
        key_head = key_heads[head_index // group_size]
        value_head = value_heads[head_index // group_size]
        scores = jnp.dot(query, key_head.T, preferred_element_type=jnp.float32) * score_scale
        row_max = lax.optimization_barrier(jnp.max(scores, axis=1, keepdims=True))
        weights = jnp.exp(scores - row_max)
        total = lax.optimization_barrier(jnp.sum(weights, axis=1, keepdims=True))
        attended = (jnp.dot(weights.astype(jnp.bfloat16), value_head, preferred_element_type=jnp.float32) / total).astype(jnp.bfloat16)
        log_total = row_max + jnp.log(total)
        d_attended = jnp.dot(out_cotangent, out_heads[head_index].T, preferred_element_type=jnp.float32).astype(jnp.bfloat16)
        delta = lax.optimization_barrier(jnp.sum(d_attended.astype(jnp.float32) * attended.astype(jnp.float32), axis=1, keepdims=True))
        probs = jnp.exp(scores - log_total)
        d_value = jnp.dot(probs.astype(jnp.bfloat16).T, d_attended, preferred_element_type=jnp.float32)
        d_probs = jnp.dot(d_attended, value_head.T, preferred_element_type=jnp.float32)
        d_scores = (probs * (d_probs - delta)).astype(jnp.bfloat16)
        d_query = jnp.dot(d_scores, key_head, preferred_element_type=jnp.float32) * score_scale
        d_key = jnp.dot(d_scores.T, query, preferred_element_type=jnp.float32) * score_scale
        return (attended, d_query, d_key, d_value)
    attended, d_query, d_key, d_value = lax.map(one_head, jnp.arange(HEADS))
    key_sum = lax.optimization_barrier(jnp.sum(d_key.reshape(KV_HEADS, group_size, SRC_ALL, HEAD_DIM), axis=1))
    value_sum = lax.optimization_barrier(jnp.sum(d_value.reshape(KV_HEADS, group_size, SRC_ALL, HEAD_DIM), axis=1))
    key_grad = key_sum.transpose(1, 0, 2).reshape(SRC_ALL, KV_HEADS * HEAD_DIM).astype(jnp.bfloat16)
    value_grad = value_sum.transpose(1, 0, 2).reshape(SRC_ALL, KV_HEADS * HEAD_DIM).astype(jnp.bfloat16)
    attended_rows = attended.transpose(1, 0, 2).reshape(TGT_ALL, HEADS * HEAD_DIM)
    query_grad = d_query.transpose(1, 0, 2).reshape(TGT_ALL, HEADS * HEAD_DIM).astype(jnp.bfloat16)
    out_weight_grad = jnp.dot(attended_rows.T, out_cotangent, preferred_element_type=jnp.float32)
    d_normed_t = jnp.dot(query_grad, query_weight.T, preferred_element_type=jnp.float32)
    target_grad = out_cotangent.astype(jnp.float32) + norm_back(target_rows, target_gain, d_normed_t)
    d_normed_s = jnp.dot(key_grad, key_weight.T, preferred_element_type=jnp.float32) + jnp.dot(value_grad, value_weight.T, preferred_element_type=jnp.float32)
    source_grad = norm_back(source_rows, source_gain, d_normed_s)
    return (target_grad, source_grad, out_weight_grad)
```

```python
import jax
import jax.numpy as jnp
from jax import lax
from jax.experimental import pallas as pl
from jax.experimental.pallas import tpu as pltpu
from jax.sharding import PartitionSpec as P

HEAD_DIM = 64
KV_HEADS = 8
EPSILON = 1e-06
STAT_ROWS = 8
LIMB_ROWS = 16


F32 = jnp.float32
BF16 = jnp.bfloat16


def normalize(matrix, gain_vector):
    widened = matrix.astype(F32)
    factor = lax.rsqrt(jnp.mean(widened * widened, axis=-1, keepdims=True) + EPSILON)
    return (widened * factor * gain_vector).astype(BF16)


def norm_back(matrix, gain_vector, upstream):
    widened = matrix.astype(F32)
    factor = lax.rsqrt(jnp.mean(widened * widened, axis=-1, keepdims=True) + EPSILON)
    weighted = upstream * gain_vector
    inner_sum = jnp.mean(weighted * widened, axis=-1, keepdims=True)
    return factor * weighted - widened * factor**3 * inner_sum


def swap(array, axis, mask):
    size = lax.axis_size(axis)
    return lax.ppermute(array, axis, [(i, i ^ mask) for i in range(size)])


def doubling(array, axis, bits):
    blocks = {0: array}
    for bit in bits:
        received = {key ^ bit: swap(value, axis, bit) for key, value in blocks.items()}
        blocks.update(received)
    return blocks


def nt_dot(a, b):
    return lax.dot_general(a, b, (((1,), (1,)), ((), ())), preferred_element_type=F32)


def tn_dot(a, b):
    return lax.dot_general(a, b, (((0,), (0,)), ((), ())), preferred_element_type=F32)


def chunk_for(rows):
    return 256 if rows % 256 == 0 else rows


def limbs_of(value):
    high = value.astype(BF16)
    rest = value - high.astype(F32)
    middle = rest.astype(BF16)
    low = (rest - middle.astype(F32)).astype(BF16)
    return high, middle, low


def forward_kernel(query_ref, kv_ref, out_ref, score_ref):
    lanes = query_ref.shape[1]
    rows = kv_ref.shape[0]
    chunk = chunk_for(rows)
    query = jnp.concatenate([query_ref[...], jnp.zeros((HEAD_DIM, lanes), BF16)], axis=0)

    def first(index, peak):
        at = pl.ds(index * chunk, chunk)
        scores = jnp.dot(kv_ref[at, :], query, preferred_element_type=F32)
        score_ref[at, :] = scores
        return jnp.maximum(peak, jnp.max(scores.reshape(chunk // 8, 8, lanes), axis=0))

    peak = lax.fori_loop(0, rows // chunk, first, jnp.full((8, lanes), -jnp.inf, F32))
    row_max = jnp.max(peak, axis=0, keepdims=True)

    def second(index, carried):
        total, summed = carried
        at = pl.ds(index * chunk, chunk)
        weights = jnp.exp(score_ref[at, :] - row_max)
        total = total + jnp.sum(weights.reshape(chunk // 8, 8, lanes), axis=0)
        summed = summed + tn_dot(kv_ref[at, :], weights.astype(BF16))
        return total, summed

    total, summed = lax.fori_loop(
        0,
        rows // chunk,
        second,
        (jnp.zeros((8, lanes), F32), jnp.zeros((2 * HEAD_DIM, lanes), F32)),
    )
    total = jnp.sum(total, axis=0, keepdims=True)
    out_ref[0:HEAD_DIM, :] = (summed[HEAD_DIM:, :] / total).astype(BF16)
    high, middle, low = limbs_of(row_max + jnp.log(total))
    place = lax.broadcasted_iota(jnp.int32, (LIMB_ROWS, lanes), 0)
    spread = jnp.where(
        place == 0,
        high.astype(F32),
        jnp.where(place == 1, middle.astype(F32), jnp.where(place == 2, low.astype(F32), 0.0)),
    )
    out_ref[HEAD_DIM:, :] = spread.astype(BF16)


def forward_block(query, kv):
    lanes = query.shape[1]
    rows = kv.shape[0]
    return pl.pallas_call(
        forward_kernel,
        out_shape=jax.ShapeDtypeStruct((HEAD_DIM + LIMB_ROWS, lanes), BF16),
        scratch_shapes=[pltpu.VMEM((rows, lanes), F32)],
        cost_estimate=pl.CostEstimate(
            flops=4 * rows * lanes * 2 * HEAD_DIM, bytes_accessed=4 * rows * 128, transcendentals=rows * lanes
        ),
        name="forward_block",
    )(query, kv)


def combine_kernel(*refs):
    parts = refs[:-3]
    grad_ref, stat_ref, attended_ref = refs[-3:]
    logs = []
    for part in parts:
        limbs = part[HEAD_DIM:, :].astype(F32)
        logs.append(limbs[0:1, :] + limbs[1:2, :] + limbs[2:3, :])
    peak = logs[0]
    for log in logs[1:]:
        peak = jnp.maximum(peak, log)
    total = jnp.zeros_like(peak)
    summed = jnp.zeros((HEAD_DIM, peak.shape[1]), F32)
    for part, log in zip(parts, logs):
        share = jnp.exp(log - peak)
        total = total + share
        summed = summed + share * part[0:HEAD_DIM, :].astype(F32)
    attended = (summed / total).astype(BF16)
    delta = jnp.sum(grad_ref[...].astype(F32) * attended.astype(F32), axis=0, keepdims=True)
    place = lax.broadcasted_iota(jnp.int32, stat_ref.shape, 0)
    stat_ref[...] = jnp.where(place == 0, peak + jnp.log(total), jnp.where(place == 1, delta, 0.0))
    attended_ref[...] = attended


def combine(parts, grad):
    lanes = grad.shape[1]
    return pl.pallas_call(
        combine_kernel,
        out_shape=(
            jax.ShapeDtypeStruct((STAT_ROWS, lanes), F32),
            jax.ShapeDtypeStruct((HEAD_DIM, lanes), BF16),
        ),
        name="combine_parts",
    )(*parts, grad)


def backward_kernel(query_ref, grad_ref, stat_ref, kv_ref, sum_in_ref, dq_ref, sum_ref):
    lanes = query_ref.shape[1]
    rows = kv_ref.shape[0]
    chunk = chunk_for(rows)
    zeros = jnp.zeros((HEAD_DIM, lanes), BF16)
    query = jnp.concatenate([query_ref[...], zeros], axis=0)
    grad = jnp.concatenate([zeros, grad_ref[...]], axis=0)
    log_total = stat_ref[0:1, :]
    delta = stat_ref[1:2, :]

    def step(index, d_query):
        at = pl.ds(index * chunk, chunk)
        kv = kv_ref[at, :]
        probs = jnp.exp(jnp.dot(kv, query, preferred_element_type=F32) - log_total)
        d_probs = jnp.dot(kv, grad, preferred_element_type=F32)
        d_scores = (probs * (d_probs - delta)).astype(BF16)
        sum_ref[at, :] = (
            sum_in_ref[at, :] + nt_dot(d_scores, query) + nt_dot(probs.astype(BF16), grad)
        )
        return d_query + tn_dot(kv, d_scores)

    d_query = lax.fori_loop(0, rows // chunk, step, jnp.zeros((2 * HEAD_DIM, lanes), F32))
    dq_ref[...] = (d_query[0:HEAD_DIM, :] * HEAD_DIM**-0.5).astype(BF16)


def backward_block(query, grad, stats, kv, sums):
    lanes = query.shape[1]
    rows = kv.shape[0]
    return pl.pallas_call(
        backward_kernel,
        out_shape=(
            jax.ShapeDtypeStruct((HEAD_DIM, lanes), BF16),
            jax.ShapeDtypeStruct((rows, 2 * HEAD_DIM), F32),
        ),
        cost_estimate=pl.CostEstimate(
            flops=10 * rows * lanes * 2 * HEAD_DIM, bytes_accessed=16 * rows * 128, transcendentals=rows * lanes
        ),
        name="backward_block",
    )(query, grad, stats, kv, sums)


def body(
    target_rows,
    source_rows,
    target_gain,
    source_gain,
    query_weight,
    key_weight,
    value_weight,
    out_weight,
    out_cotangent,
):
    tp_count = lax.axis_size("tp")
    sp_count = lax.axis_size("sp")
    tp_at = lax.axis_index("tp")
    own_rows, width = target_rows.shape
    own_source = source_rows.shape[0]
    weight_rows = key_weight.shape[0]
    local_heads = query_weight.shape[1] // HEAD_DIM
    copies = max(1, tp_count // KV_HEADS)
    block_rows = own_rows * tp_count
    lanes = local_heads * block_rows
    chips = tp_count // 2
    chip_bits = [1 << b for b in range(1, tp_count.bit_length() - 1)]
    near, far = chip_bits[: len(chip_bits) // 2], chip_bits[len(chip_bits) // 2 :]
    chip_masks = range(0, tp_count, 2)

    normed_t = normalize(target_rows, target_gain)
    normed_s = normalize(source_rows, source_gain)

    halves = jnp.concatenate(
        [normed_t if m == 0 else swap(normed_t, "tp", m) for m in chip_masks], axis=0
    )
    normed_block = jnp.concatenate([halves, swap(halves, "tp", 1)], axis=0)

    key_blocks = doubling(key_weight, "tp", far + near)
    value_blocks = doubling(value_weight, "tp", near + far)

    def whole_weight(blocks):
        full = jnp.zeros((weight_rows * tp_count, KV_HEADS * HEAD_DIM), BF16)
        for mask in chip_masks:
            mine = blocks[mask]
            other = swap(mine, "tp", 1)
            full = lax.dynamic_update_slice_in_dim(full, mine, (tp_at ^ mask) * weight_rows, 0)
            full = lax.dynamic_update_slice_in_dim(full, other, (tp_at ^ mask ^ 1) * weight_rows, 0)
        return full

    key_full = whole_weight(key_blocks)
    value_full = whole_weight(value_blocks)

    cot_z = jnp.stack(
        [out_cotangent if k == 0 else swap(out_cotangent, "sp", k) for k in range(sp_count)]
    )
    cot_half = jnp.stack([cot_z if m == 0 else swap(cot_z, "tp", m) for m in chip_masks])
    cot_all = jnp.stack([cot_half, swap(cot_half, "tp", 1)])
    cot_all = cot_all.transpose(2, 0, 1, 3, 4).reshape(sp_count * block_rows, width)

    def stacked(transposed):
        rows = transposed.shape[1]
        split = transposed.reshape(local_heads, HEAD_DIM, rows)
        return split.transpose(1, 0, 2).reshape(HEAD_DIM, local_heads * rows)

    def unstacked(array):
        split = array.reshape(HEAD_DIM, local_heads, block_rows)
        return split.transpose(1, 0, 2).reshape(local_heads * HEAD_DIM, block_rows)

    queries = lax.dot_general(
        query_weight, normed_block, (((0,), (1,)), ((), ())), preferred_element_type=F32
    ).astype(BF16)
    queries = stacked(queries) * jnp.asarray(HEAD_DIM**-0.5, BF16)
    all_queries = [queries if k == 0 else swap(queries, "sp", k) for k in range(sp_count)]

    d_attended = nt_dot(out_weight, cot_all).astype(BF16)
    all_grads = [
        stacked(d_attended[:, k * block_rows : (k + 1) * block_rows]) for k in range(sp_count)
    ]

    keys = jnp.dot(normed_s, key_full, preferred_element_type=F32).astype(BF16)
    values = jnp.dot(normed_s, value_full, preferred_element_type=F32).astype(BF16)
    packed = jnp.concatenate(
        [
            keys.reshape(own_source, KV_HEADS, HEAD_DIM),
            values.reshape(own_source, KV_HEADS, HEAD_DIM),
        ],
        axis=-1,
    ).transpose(1, 0, 2)
    packed = jnp.repeat(packed, copies, axis=0)
    kv = lax.all_to_all(packed, "tp", split_axis=0, concat_axis=0, tiled=True)
    kv = kv.reshape(tp_count * own_source, 2 * HEAD_DIM)

    order = list(range(sp_count // 2, sp_count)) + list(range(sp_count // 2 - 1, -1, -1))
    parts = []
    for k in order:
        part = forward_block(all_queries[k], kv)
        parts.append(part if k == 0 else swap(part, "sp", k))
    stats, attended = combine(parts, all_grads[0])
    all_stats = [stats if k == 0 else swap(stats, "sp", k) for k in range(sp_count)]
    attended = unstacked(attended)
    all_attended = jnp.concatenate(
        [attended if k == 0 else swap(attended, "sp", k) for k in range(sp_count)], axis=1
    )

    sums = jnp.zeros((tp_count * own_source, 2 * HEAD_DIM), F32)
    query_grad = jnp.zeros((HEAD_DIM, lanes), F32)
    for k in order:
        d_query, sums = backward_block(all_queries[k], all_grads[k], all_stats[k], kv, sums)
        query_grad = query_grad + (d_query if k == 0 else swap(d_query, "sp", k)).astype(F32)
    query_grad = unstacked(query_grad.astype(BF16))

    back = lax.all_to_all(
        sums.astype(BF16).reshape(tp_count, own_source, 2 * HEAD_DIM),
        "tp",
        split_axis=0,
        concat_axis=0,
        tiled=True,
    )
    if copies > 1:
        back = back.reshape(KV_HEADS, copies, own_source, 2 * HEAD_DIM).astype(F32).sum(1).astype(BF16)
    back = back.transpose(1, 0, 2)
    key_grad = back[:, :, :HEAD_DIM].reshape(own_source, KV_HEADS * HEAD_DIM)
    value_grad = back[:, :, HEAD_DIM:].reshape(own_source, KV_HEADS * HEAD_DIM)
    d_normed_s = nt_dot(key_grad, key_full) + nt_dot(value_grad, value_full)
    source_grad = norm_back(source_rows, source_gain, d_normed_s)

    d_normed_t = lax.dot_general(
        query_grad, query_weight, (((0,), (1,)), ((), ())), preferred_element_type=F32
    ).reshape(2, chips * own_rows, width)
    mine = d_normed_t[0] + swap(d_normed_t[1].astype(BF16), "tp", 1).astype(F32)
    mine = mine.reshape(chips, own_rows, width)
    total = mine[0]
    for at, m in enumerate(chip_masks):
        if m:
            total = total + swap(mine[at].astype(BF16), "tp", m).astype(F32)
    target_grad = out_cotangent.astype(F32) + norm_back(target_rows, target_gain, total)

    out_weight_grad = jnp.dot(all_attended, cot_all, preferred_element_type=F32)
    return (target_grad, source_grad, out_weight_grad)


def solution(mesh):
    return jax.shard_map(
        body,
        mesh=mesh,
        in_specs=(
            P(("sp", "tp"), None),
            P(("sp", "tp"), None),
            P(),
            P(),
            P(None, "tp"),
            P("tp", None),
            P("tp", None),
            P("tp", None),
            P(("sp", "tp"), None),
        ),
        out_specs=(P(("sp", "tp"), None), P(("sp", "tp"), None), P("tp", None)),
        check_vma=False,
    )
```

```python
import jax
import jax.numpy as jnp
from jax import lax
from jax.experimental import pallas as pl
from jax.experimental.pallas import tpu as pltpu
from jax.sharding import PartitionSpec as P


HEAD_DIM = 64
KV_HEADS = 8
EPSILON = 1e-06
SCALE = HEAD_DIM**-0.5


F32 = jnp.float32
BF16 = jnp.bfloat16


def shape_of(shape, dtype):
    return jax.ShapeDtypeStruct(shape, dtype)


def normalize(matrix, gain_vector):
    widened = matrix.astype(F32)
    factor = lax.rsqrt(jnp.mean(widened * widened, axis=-1, keepdims=True) + EPSILON)
    return (widened * factor * gain_vector).astype(BF16)


def norm_back(matrix, gain_vector, upstream):
    widened = matrix.astype(F32)
    factor = lax.rsqrt(jnp.mean(widened * widened, axis=-1, keepdims=True) + EPSILON)
    weighted = upstream * gain_vector
    inner_sum = jnp.mean(weighted * widened, axis=-1, keepdims=True)
    return factor * weighted - widened * factor**3 * inner_sum


def swap(array, axis, mask):
    size = lax.axis_size(axis)
    return lax.ppermute(array, axis, [(i, i ^ mask) for i in range(size)])


def doubling(array, axis, bits):
    blocks = {0: array}
    for bit in bits:
        received = {key ^ bit: swap(value, axis, bit) for key, value in blocks.items()}
        blocks.update(received)
    return blocks


def dot(a, b):
    return jnp.dot(a, b, preferred_element_type=F32)


def nt_dot(a, b):
    return lax.dot_general(a, b, (((1,), (1,)), ((), ())), preferred_element_type=F32)


def tn_dot(a, b):
    return lax.dot_general(a, b, (((0,), (0,)), ((), ())), preferred_element_type=F32)


def chunk_for(rows):
    return 256 if rows % 256 == 0 else rows


def pad_to(extent, multiple):
    return -(-extent // multiple) * multiple


def transposed(matrix):
    rows, columns = matrix.shape
    more_rows, more_columns = pad_to(rows, 128) - rows, pad_to(columns, 128) - columns
    if more_columns:
        matrix = jnp.concatenate([matrix, jnp.zeros((rows, more_columns), F32)], axis=1)
    if more_rows:
        filler = jnp.zeros((more_rows, columns + more_columns), F32)
        matrix = jnp.concatenate([matrix, filler], axis=0)
    return matrix.T[:columns, :rows]


def stacked(matrix):
    heads = matrix.shape[0] // HEAD_DIM
    pieces = [matrix[g * HEAD_DIM : (g + 1) * HEAD_DIM, :] for g in range(heads)]
    return jnp.concatenate(pieces, axis=1) if heads > 1 else pieces[0]


def unstacked(matrix, heads):
    rows = matrix.shape[1] // heads
    pieces = [matrix[:, g * rows : (g + 1) * rows] for g in range(heads)]
    return jnp.concatenate(pieces, axis=0) if heads > 1 else pieces[0]


SCALAR = pl.BlockSpec(memory_space=pltpu.SMEM)
WHOLE = pl.BlockSpec(memory_space=pltpu.VMEM)


def split_norm(tp_at, source_rows, gain, weight_rows, tp_count):
    rows, width = source_rows.shape
    half = width // 2
    masks = range(0, tp_count, 2)
    if weight_rows % 128:
        normed = normalize(source_rows, gain)

        def columns(parity):
            return jnp.concatenate(
                [
                    lax.dynamic_slice_in_dim(
                        normed, (tp_at ^ m ^ parity) * weight_rows, weight_rows, 1
                    )
                    for m in masks
                ],
                axis=1,
            )

        return columns(0), columns(1)

    def kernel(at_ref, rows_ref, gain_ref, own_ref, other_ref):
        widened = rows_ref[...].astype(F32)
        factor = lax.rsqrt(jnp.mean(widened * widened, axis=-1, keepdims=True) + EPSILON)
        for parity, out_ref in ((0, own_ref), (1, other_ref)):
            for place, m in enumerate(masks):
                start = pl.multiple_of((at_ref[0] ^ (m + parity)) * weight_rows, 128)
                at = pl.ds(start, weight_rows)
                piece = rows_ref[:, at].astype(F32) * factor * gain_ref[:, at]
                out_ref[:, place * weight_rows : (place + 1) * weight_rows] = piece.astype(BF16)

    return pl.pallas_call(
        kernel,
        out_shape=(shape_of((rows, half), BF16), shape_of((rows, half), BF16)),
        in_specs=[SCALAR, WHOLE, WHOLE],
        cost_estimate=pl.CostEstimate(flops=8 * rows * width, bytes_accessed=4 * rows * width, transcendentals=0),
        name="split_norm",
    )(tp_at[None], source_rows, gain[None])


def project_kv(own, other, key_blocks, value_blocks):
    rows = own.shape[0]
    count = len(key_blocks)
    weight_rows, kv_width = key_blocks[0].shape

    def kernel(own_ref, other_ref, *refs):
        keys, values = refs[:count], refs[count : 2 * count]
        near_ref, far_ref = refs[-2:]
        lhs = jnp.concatenate([own_ref[...], other_ref[...]], axis=0)
        sums = []
        for weights in (keys, values):
            total = None
            for place, weight in enumerate(weights):
                term = dot(lhs[:, place * weight_rows : (place + 1) * weight_rows], weight[...])
                total = term if total is None else total + term
            sums.append(total)
        for head in range(KV_HEADS):
            at = slice(head * HEAD_DIM, (head + 1) * HEAD_DIM)
            packed = jnp.concatenate([sums[0][:, at], sums[1][:, at]], axis=1)
            near_ref[head] = packed[:rows]
            far_ref[head] = packed[rows:]

    return pl.pallas_call(
        kernel,
        out_shape=(shape_of((KV_HEADS, rows, 2 * HEAD_DIM), F32),) * 2,
        cost_estimate=pl.CostEstimate(
            flops=8 * rows * count * weight_rows * kv_width,
            bytes_accessed=4 * count * weight_rows * kv_width,
            transcendentals=0,
        ),
        name="project_kv",
    )(own, other, *key_blocks, *value_blocks)


def project_queries(pieces, query_weight):
    count = sum(piece.shape[0] for piece in pieces)
    heads = query_weight.shape[1] // HEAD_DIM

    def kernel(*refs):
        piece_refs, weight_ref, out_ref = refs[:-2], refs[-2], refs[-1]
        rows = jnp.concatenate([ref[...] for ref in piece_refs], axis=0)
        queries = dot(rows, weight_ref[...])
        out_ref[...] = stacked(transposed(queries)).astype(BF16) * jnp.asarray(SCALE, BF16)

    return pl.pallas_call(
        kernel,
        out_shape=shape_of((HEAD_DIM, heads * count), BF16),
        cost_estimate=pl.CostEstimate(
            flops=2 * count * query_weight.size, bytes_accessed=2 * query_weight.size, transcendentals=0
        ),
        name="project_queries",
    )(*pieces, query_weight)


def project_grads(pieces, out_weight):
    blocks, piece_rows, width = pieces[0].shape
    count = piece_rows * len(pieces)
    heads = out_weight.shape[0] // HEAD_DIM

    def kernel(*refs):
        piece_refs, weight_ref, out_ref, cot_ref = refs[:-3], refs[-3], refs[-2], refs[-1]
        for block in range(blocks):
            rows = jnp.concatenate([ref[block] for ref in piece_refs], axis=0)
            cot_ref[block * count : (block + 1) * count, :] = rows
            out_ref[block] = stacked(nt_dot(weight_ref[...], rows)).astype(BF16)

    return pl.pallas_call(
        kernel,
        out_shape=(
            shape_of((blocks, HEAD_DIM, heads * count), BF16),
            shape_of((blocks * count, width), BF16),
        ),
        cost_estimate=pl.CostEstimate(
            flops=2 * blocks * count * out_weight.size, bytes_accessed=2 * blocks * count * width, transcendentals=0
        ),
        name="project_grads",
    )(*pieces, out_weight)


def forward_all(queries, grads, kv):
    blocks = len(queries)
    lanes = queries[0].shape[1]
    rows = kv.shape[0]
    chunk = chunk_for(rows)

    def kernel(*refs):
        query_refs, (grad_ref, kv_ref) = refs[:blocks], refs[blocks : blocks + 2]
        out_ref, stat_ref, score_ref = refs[blocks + 2 :]
        zeros = jnp.zeros((HEAD_DIM, lanes), BF16)
        for block, query_ref in enumerate(query_refs):
            query = jnp.concatenate([query_ref[...], zeros], axis=0)
            slot = block % 2
            peak = jnp.full((8, lanes), -jnp.inf, F32)
            for start in range(0, rows, chunk):
                scores = dot(kv_ref[start : start + chunk, :], query)
                score_ref[slot, start : start + chunk, :] = scores
                peak = jnp.maximum(peak, jnp.max(scores.reshape(chunk // 8, 8, lanes), axis=0))
            row_max = jnp.max(peak, axis=0, keepdims=True)
            total = jnp.zeros((8, lanes), F32)
            summed = jnp.zeros((HEAD_DIM, lanes), F32)
            for start in range(0, rows, chunk):
                weights = jnp.exp(score_ref[slot, start : start + chunk, :] - row_max)
                total = total + jnp.sum(weights.reshape(chunk // 8, 8, lanes), axis=0)
                values = kv_ref[start : start + chunk, HEAD_DIM:]
                summed = summed + tn_dot(values, weights.astype(BF16))
            total = jnp.sum(total, axis=0, keepdims=True)
            part = summed / total
            out_ref[block] = part
            stat_ref[2 * block : 2 * block + 1, :] = row_max + jnp.log(total)
            stat_ref[2 * block + 1 : 2 * block + 2, :] = jnp.sum(
                grad_ref[block].astype(F32) * part, axis=0, keepdims=True
            )

    return pl.pallas_call(
        kernel,
        out_shape=(
            shape_of((blocks, HEAD_DIM, lanes), F32),
            shape_of((2 * blocks, lanes), F32),
        ),
        scratch_shapes=[pltpu.VMEM((2, rows, lanes), F32)],
        cost_estimate=pl.CostEstimate(
            flops=8 * blocks * rows * lanes * HEAD_DIM,
            bytes_accessed=4 * blocks * rows * HEAD_DIM,
            transcendentals=blocks * rows * lanes,
        ),
        name="forward_all",
    )(*queries, grads, kv)


def combine_stats(stats, parts):
    blocks, _, lanes = parts.shape

    def kernel(*refs):
        stat_refs, part_ref, out_ref, share_ref = refs[:blocks], refs[blocks], refs[-2], refs[-1]
        for block in range(blocks):
            logs, deltas = [], []
            for peer, stat_ref in enumerate(stat_refs):
                at = 2 * (block ^ peer)
                logs.append(stat_ref[at : at + 1, :])
                deltas.append(stat_ref[at + 1 : at + 2, :])
            peak = logs[0]
            for log in logs[1:]:
                peak = jnp.maximum(peak, log)
            shares = [jnp.exp(log - peak) for log in logs]
            total = shares[0]
            delta = shares[0] * deltas[0]
            for share, term in zip(shares[1:], deltas[1:]):
                total = total + share
                delta = delta + share * term
            out_ref[2 * block : 2 * block + 1, :] = peak + jnp.log(total)
            out_ref[2 * block + 1 : 2 * block + 2, :] = delta / total
            share_ref[block] = (part_ref[block] * (shares[0] / total)).astype(BF16)

    return pl.pallas_call(
        kernel,
        out_shape=(
            shape_of((2 * blocks, lanes), F32),
            shape_of((blocks, HEAD_DIM, lanes), BF16),
        ),
        name="combine_stats",
    )(*stats, parts)


def backward_some(order, queries, grads, stats, kv, sums, sum_type):
    count = len(order)
    lanes = queries[0].shape[1]
    rows = kv.shape[0]
    chunk = chunk_for(rows)
    started = [] if sums is None else [sums]

    def kernel(*refs):
        query_refs = refs[:count]
        grad_ref, stat_ref, kv_ref = refs[count : count + 3]
        start_refs = refs[count + 3 : count + 3 + len(started)]
        outs = refs[count + 3 + len(started) : -1]
        sum_ref = refs[-1]
        zeros = jnp.zeros((HEAD_DIM, lanes), BF16)
        for place, block in enumerate(order):
            query = jnp.concatenate([query_refs[place][...], zeros], axis=0)
            grad = jnp.concatenate([zeros, grad_ref[block]], axis=0)
            log_total = stat_ref[2 * block : 2 * block + 1, :]
            delta = stat_ref[2 * block + 1 : 2 * block + 2, :]
            d_query = jnp.zeros((HEAD_DIM, lanes), F32)
            for start in range(0, rows, chunk):
                at = slice(start, start + chunk)
                pair = kv_ref[at, :]
                probs = jnp.exp(dot(pair, query) - log_total)
                d_scores = (probs * (dot(pair, grad) - delta)).astype(BF16)
                terms = nt_dot(d_scores, query) + nt_dot(probs.astype(BF16), grad)
                if place:
                    terms = terms + sum_ref[at, :]
                elif started:
                    terms = terms + start_refs[0][at, :]
                sum_ref[at, :] = terms
                d_query = d_query + tn_dot(pair[:, :HEAD_DIM], d_scores)
            outs[place][...] = (d_query * SCALE).astype(BF16)
        outs[-1][...] = sum_ref[...].astype(sum_type)

    outs = pl.pallas_call(
        kernel,
        out_shape=tuple(shape_of((HEAD_DIM, lanes), BF16) for _ in order)
        + (shape_of((rows, 2 * HEAD_DIM), sum_type),),
        scratch_shapes=[pltpu.VMEM((rows, 2 * HEAD_DIM), F32)],
        cost_estimate=pl.CostEstimate(
            flops=20 * count * rows * lanes * HEAD_DIM,
            bytes_accessed=8 * count * rows * HEAD_DIM,
            transcendentals=count * rows * lanes,
        ),
        name="backward_some",
    )(*[queries[block] for block in order], grads, stats, kv, *started)
    return outs[:-1], outs[-1]


def query_back(parts, query_weight, heads):
    width = query_weight.shape[0]
    count = parts[0].shape[1] // heads
    half = count // 2

    def kernel(*refs):
        part_refs, weight_ref, own_ref, other_ref = refs[:-3], refs[-3], refs[-2], refs[-1]
        total = part_refs[0][...].astype(F32)
        for part_ref in part_refs[1:]:
            total = total + part_ref[...].astype(F32)
        grad = transposed(unstacked(total, heads)).astype(BF16)
        upstream = nt_dot(grad, weight_ref[...])
        own_ref[...] = upstream[:half]
        other_ref[...] = upstream[half:].astype(BF16)

    return pl.pallas_call(
        kernel,
        out_shape=(shape_of((half, width), F32), shape_of((half, width), BF16)),
        cost_estimate=pl.CostEstimate(
            flops=2 * count * query_weight.size, bytes_accessed=2 * query_weight.size, transcendentals=0
        ),
        name="query_back",
    )(*parts, query_weight)


def share_rows(own, theirs, count):
    rows, width = own.shape
    piece = rows // count

    def kernel(own_ref, theirs_ref, kept_ref, *out_refs):
        kept_ref[...] = own_ref[:piece, :] + theirs_ref[:piece, :].astype(F32)
        for place, out_ref in enumerate(out_refs):
            at = slice((place + 1) * piece, (place + 2) * piece)
            out_ref[...] = (own_ref[at, :] + theirs_ref[at, :].astype(F32)).astype(BF16)

    return pl.pallas_call(
        kernel,
        out_shape=(shape_of((piece, width), F32),)
        + tuple(shape_of((piece, width), BF16) for _ in range(count - 1)),
        name="share_rows",
    )(own, theirs)


def target_finish(kept, received, target_rows, cotangent, gain):
    def kernel(kept_ref, *refs):
        received_refs, (rows_ref, cot_ref, gain_ref, out_ref) = refs[:-4], refs[-4:]
        total = kept_ref[...]
        for ref in received_refs:
            total = total + ref[...].astype(F32)
        back = norm_back(rows_ref[...], gain_ref[...], total)
        out_ref[...] = cot_ref[...].astype(F32) + back

    return pl.pallas_call(
        kernel,
        out_shape=shape_of(kept.shape, F32),
        name="target_finish",
    )(kept, *received, target_rows, cotangent, gain[None])


def attend_sum(parts):
    def kernel(*refs):
        own_ref, out_ref = refs[0], refs[-1]
        total = own_ref[0].astype(F32)
        for ref in refs[1:-1]:
            total = total + ref[...].astype(F32)
        out_ref[...] = total.astype(BF16)

    return pl.pallas_call(
        kernel, out_shape=shape_of(parts[0].shape[1:], BF16), name="attend_sum"
    )(*parts)


def weight_grad(attended, cot_all, heads):
    blocks = len(attended)
    count = cot_all.shape[0] // blocks
    width = cot_all.shape[1]
    step = 512 if width % 512 == 0 else width

    def kernel(*refs):
        attended_refs, cot_ref, out_ref, wide_ref = refs[:blocks], refs[-3], refs[-2], refs[-1]

        @pl.when(pl.program_id(0) == 0)
        def _():
            for block, attended_ref in enumerate(attended_refs):
                wide_ref[block] = unstacked(attended_ref[...].astype(F32), heads).astype(BF16)

        total = None
        for block in range(blocks):
            term = dot(wide_ref[block], cot_ref[block * count : (block + 1) * count, :])
            total = term if total is None else total + term
        out_ref[...] = total

    part_spec = pl.BlockSpec(attended[0].shape, lambda i: (0, 0))
    return pl.pallas_call(
        kernel,
        grid=(width // step,),
        in_specs=[part_spec] * blocks + [pl.BlockSpec((cot_all.shape[0], step), lambda i: (0, i))],
        out_specs=pl.BlockSpec((heads * HEAD_DIM, step), lambda i: (0, i)),
        out_shape=shape_of((heads * HEAD_DIM, width), F32),
        scratch_shapes=[pltpu.VMEM((blocks, heads * HEAD_DIM, count), BF16)],
        cost_estimate=pl.CostEstimate(
            flops=2 * heads * HEAD_DIM * cot_all.size, bytes_accessed=2 * cot_all.size, transcendentals=0
        ),
        name="weight_grad",
    )(*attended, cot_all)


def source_back(tp_at, back, key_blocks, value_blocks, others, source_rows, gain):
    rows, width = source_rows.shape
    count = len(key_blocks)
    weight_rows = key_blocks[0].shape[0]

    def kernel(at_ref, back_ref, *refs):
        keys, values = refs[:count], refs[count : 2 * count]
        other_ref, rows_ref, gain_ref, out_ref = refs[2 * count :]
        key_grad = jnp.concatenate([back_ref[h][:, :HEAD_DIM] for h in range(KV_HEADS)], axis=1)
        value_grad = jnp.concatenate([back_ref[h][:, HEAD_DIM:] for h in range(KV_HEADS)], axis=1)
        inner = jnp.zeros((rows, 1), F32)
        square = jnp.zeros((rows, 1), F32)
        for place in range(count):
            for parity in (0, 1):
                if parity:
                    key, value = other_ref[0, place], other_ref[1, place]
                else:
                    key, value = keys[place][...], values[place][...]
                start = pl.multiple_of((at_ref[0] ^ (2 * place + parity)) * weight_rows, 128)
                at = pl.ds(start, weight_rows)
                weighted = (nt_dot(key_grad, key) + nt_dot(value_grad, value)) * gain_ref[:, at]
                widened = rows_ref[:, at].astype(F32)
                inner = inner + jnp.sum(weighted * widened, axis=-1, keepdims=True)
                square = square + jnp.sum(widened * widened, axis=-1, keepdims=True)
                out_ref[:, at] = weighted
        factor = lax.rsqrt(square / width + EPSILON)
        pull = factor**3 * (inner / width)
        out_ref[...] = factor * out_ref[...] - rows_ref[...].astype(F32) * pull

    return pl.pallas_call(
        kernel,
        out_shape=shape_of((rows, width), F32),
        in_specs=[SCALAR] + [WHOLE] * (2 * count + 4),
        cost_estimate=pl.CostEstimate(
            flops=4 * rows * width * KV_HEADS * HEAD_DIM,
            bytes_accessed=4 * width * KV_HEADS * HEAD_DIM,
            transcendentals=0,
        ),
        name="source_back",
    )(tp_at[None], back, *key_blocks, *value_blocks, others, source_rows, gain[None])


def source_back_plain(tp_at, back, key_blocks, value_blocks, others, source_rows, gain):
    rows, width = source_rows.shape
    weight_rows = key_blocks[0].shape[0]
    total = jnp.zeros((rows, width), F32)
    fulls = []
    for kind, blocks in enumerate((key_blocks, value_blocks)):
        full = jnp.zeros((width, KV_HEADS * HEAD_DIM), BF16)
        for place, block in enumerate(blocks):
            start = (tp_at ^ (2 * place)) * weight_rows
            full = lax.dynamic_update_slice_in_dim(full, block, start, 0)
            start = (tp_at ^ (2 * place + 1)) * weight_rows
            full = lax.dynamic_update_slice_in_dim(full, others[kind, place], start, 0)
        fulls.append(full)
    turned = back.transpose(1, 0, 2)
    key_grad = turned[:, :, :HEAD_DIM].reshape(rows, KV_HEADS * HEAD_DIM)
    value_grad = turned[:, :, HEAD_DIM:].reshape(rows, KV_HEADS * HEAD_DIM)
    total = nt_dot(key_grad, fulls[0]) + nt_dot(value_grad, fulls[1])
    return norm_back(source_rows, gain, total)


def body(
    target_rows,
    source_rows,
    target_gain,
    source_gain,
    query_weight,
    key_weight,
    value_weight,
    out_weight,
    out_cotangent,
):
    tp_count = lax.axis_size("tp")
    sp_count = lax.axis_size("sp")
    tp_at = lax.axis_index("tp").astype(jnp.int32)
    own_source = source_rows.shape[0]
    weight_rows = key_weight.shape[0]
    heads = query_weight.shape[1] // HEAD_DIM
    copies = max(1, tp_count // KV_HEADS)
    chips = tp_count // 2
    chip_bits = [1 << b for b in range(1, tp_count.bit_length() - 1)]
    near, far = chip_bits[: len(chip_bits) // 2], chip_bits[len(chip_bits) // 2 :]
    chip_masks = range(0, tp_count, 2)

    normed_t = normalize(target_rows, target_gain)
    near_rows = [normed_t if m == 0 else swap(normed_t, "tp", m) for m in chip_masks]
    far_rows = [swap(rows, "tp", 1) for rows in near_rows]
    queries = project_queries(near_rows + far_rows, query_weight)
    all_queries = [queries if k == 0 else swap(queries, "sp", k) for k in range(sp_count)]

    key_found = doubling(key_weight, "tp", far + near)
    value_found = doubling(value_weight, "tp", near + far)
    key_blocks = [key_found[m] for m in chip_masks]
    value_blocks = [value_found[m] for m in chip_masks]

    own_part, other_part = split_norm(tp_at, source_rows, source_gain, weight_rows, tp_count)
    other_part = swap(other_part, "tp", 1)
    own_sum, other_sum = project_kv(own_part, other_part, key_blocks, value_blocks)
    packed = (own_sum + swap(other_sum, "tp", 1)).astype(BF16)
    packed = jnp.repeat(packed, copies, axis=0)
    kv = lax.all_to_all(packed, "tp", split_axis=0, concat_axis=0, tiled=True)
    kv = kv.reshape(tp_count * own_source, 2 * HEAD_DIM)

    cot_z = jnp.stack(
        [out_cotangent if k == 0 else swap(out_cotangent, "sp", k) for k in range(sp_count)]
    )
    cot_near = [cot_z if m == 0 else swap(cot_z, "tp", m) for m in chip_masks]
    cot_far = [swap(rows, "tp", 1) for rows in cot_near]
    all_grads, cot_all = project_grads(cot_near + cot_far, out_weight)

    parts, own_stats = forward_all(all_queries, all_grads, kv)
    stats = [own_stats if k == 0 else swap(own_stats, "sp", k) for k in range(sp_count)]
    stats, shares = combine_stats(stats, parts)
    order = list(range(sp_count // 2, sp_count)) + list(range(sp_count // 2 - 1, -1, -1))
    first, second = order[: sp_count // 2], order[sp_count // 2 :]
    found, kv_sums = backward_some(first, all_queries, all_grads, stats, kv, None, F32)
    query_parts = [swap(part, "sp", k) for k, part in zip(first, found)]
    found, kv_sums = backward_some(second, all_queries, all_grads, stats, kv, kv_sums, BF16)
    query_parts += [part if k == 0 else swap(part, "sp", k) for k, part in zip(second, found)]

    others = jnp.stack([jnp.stack(key_blocks), jnp.stack(value_blocks)])
    others = swap(others, "tp", 1)
    back = lax.all_to_all(
        kv_sums.reshape(tp_count, own_source, 2 * HEAD_DIM),
        "tp",
        split_axis=0,
        concat_axis=0,
        tiled=True,
    )
    if copies > 1:
        back = back.reshape(KV_HEADS, copies, own_source, 2 * HEAD_DIM)
        back = back.astype(F32).sum(1).astype(BF16)
    finish = source_back_plain if weight_rows % 128 else source_back
    source_grad = finish(tp_at, back, key_blocks, value_blocks, others, source_rows, source_gain)

    mine, theirs = query_back(query_parts, query_weight, heads)
    theirs = swap(theirs, "tp", 1)
    kept, *given = share_rows(mine, theirs, chips)
    received = [swap(piece, "tp", m) for m, piece in zip(list(chip_masks)[1:], given)]
    target_grad = target_finish(kept, received, target_rows, out_cotangent, target_gain)

    attended = [shares] + [swap(shares[k], "sp", k) for k in range(1, sp_count)]
    attended = attend_sum(attended)
    attended = [attended if k == 0 else swap(attended, "sp", k) for k in range(sp_count)]
    out_weight_grad = weight_grad(attended, cot_all, heads)
    return (target_grad, source_grad, out_weight_grad)


def solution(mesh):
    return jax.shard_map(
        body,
        mesh=mesh,
        in_specs=(
            P(("sp", "tp"), None),
            P(("sp", "tp"), None),
            P(),
            P(),
            P(None, "tp"),
            P("tp", None),
            P("tp", None),
            P("tp", None),
            P(("sp", "tp"), None),
        ),
        out_specs=(P(("sp", "tp"), None), P(("sp", "tp"), None), P("tp", None)),
        check_vma=False,
    )
```

```python
import jax
import jax.numpy as jnp
from jax import lax
from jax.experimental import pallas as pl
from jax.experimental.pallas import tpu as pltpu
from jax.sharding import PartitionSpec as P


HEAD_DIM = 64
KV_HEADS = 8
EPSILON = 1e-06
SCALE = HEAD_DIM**-0.5


F32 = jnp.float32
BF16 = jnp.bfloat16


def shape_of(shape, dtype):
    return jax.ShapeDtypeStruct(shape, dtype)


def normalize(matrix, gain_vector):
    widened = matrix.astype(F32)
    factor = lax.rsqrt(jnp.mean(widened * widened, axis=-1, keepdims=True) + EPSILON)
    return (widened * factor * gain_vector).astype(BF16)


def norm_back(matrix, gain_vector, upstream):
    widened = matrix.astype(F32)
    factor = lax.rsqrt(jnp.mean(widened * widened, axis=-1, keepdims=True) + EPSILON)
    weighted = upstream * gain_vector
    inner_sum = jnp.mean(weighted * widened, axis=-1, keepdims=True)
    return factor * weighted - widened * factor**3 * inner_sum


def swap(array, axis, mask):
    size = lax.axis_size(axis)
    return lax.ppermute(array, axis, [(i, i ^ mask) for i in range(size)])


def doubling(array, axis, bits):
    blocks = {0: array}
    for bit in bits:
        received = {key ^ bit: swap(value, axis, bit) for key, value in blocks.items()}
        blocks.update(received)
    return blocks


def dot(a, b):
    return jnp.dot(a, b, preferred_element_type=F32)


def nt_dot(a, b):
    return lax.dot_general(a, b, (((1,), (1,)), ((), ())), preferred_element_type=F32)


def tn_dot(a, b):
    return lax.dot_general(a, b, (((0,), (0,)), ((), ())), preferred_element_type=F32)


def chunk_for(rows):
    return 256 if rows % 256 == 0 else rows


def pad_to(extent, multiple):
    return -(-extent // multiple) * multiple


def transposed(matrix):
    rows, columns = matrix.shape
    more_rows, more_columns = pad_to(rows, 128) - rows, pad_to(columns, 128) - columns
    if more_columns:
        matrix = jnp.concatenate([matrix, jnp.zeros((rows, more_columns), F32)], axis=1)
    if more_rows:
        filler = jnp.zeros((more_rows, columns + more_columns), F32)
        matrix = jnp.concatenate([matrix, filler], axis=0)
    return matrix.T[:columns, :rows]


def stacked(matrix):
    heads = matrix.shape[0] // HEAD_DIM
    pieces = [matrix[g * HEAD_DIM : (g + 1) * HEAD_DIM, :] for g in range(heads)]
    return jnp.concatenate(pieces, axis=1) if heads > 1 else pieces[0]


def unstacked(matrix, heads):
    rows = matrix.shape[1] // heads
    pieces = [matrix[:, g * rows : (g + 1) * rows] for g in range(heads)]
    return jnp.concatenate(pieces, axis=0) if heads > 1 else pieces[0]


SCALAR = pl.BlockSpec(memory_space=pltpu.SMEM)
WHOLE = pl.BlockSpec(memory_space=pltpu.VMEM)
ROOM = 16 << 20


def resident(
    kernel,
    out_shape,
    *args,
    scalar=None,
    kept=None,
    loaded=0,
    fetched=0,
    far=0,
    scratch=(),
    room=ROOM,
    **costs,
):
    single = not isinstance(out_shape, tuple)
    outs = (out_shape,) if single else out_shape
    kept = len(outs) if kept is None else kept
    outs = tuple(
        (pltpu.VMEM if at < kept else pltpu.HBM)(out.shape, out.dtype)
        for at, out in enumerate(outs)
    )
    near = len(args) - far
    specs = [WHOLE] * near + [pl.BlockSpec(memory_space=pltpu.HBM)] * far
    held = near - fetched

    def placed(at, arg):
        if at < held - loaded:
            return pltpu.with_memory_space_constraint(arg, pltpu.VMEM)
        return arg if at < held else pltpu.with_memory_space_constraint(arg, pltpu.HBM)

    args = [placed(at, arg) for at, arg in enumerate(args)]
    if scalar is not None:
        args, specs = [scalar[None]] + args, [SCALAR] + specs
    return pl.pallas_call(
        kernel,
        out_shape=outs[0] if single else outs,
        in_specs=specs,
        out_specs=WHOLE if single else (WHOLE,) * len(outs),
        scratch_shapes=list(scratch),
        cost_estimate=pl.CostEstimate(
            flops=costs.get("flops", 1 << 20),
            bytes_accessed=costs.get("moved", 1 << 20),
            transcendentals=costs.get("exps", 0),
        ),
        compiler_params=pltpu.CompilerParams(vmem_limit_bytes=room),
    )(*args)


def split_norm(tp_at, source_rows, gain, weight_rows, tp_count, carried):
    rows, width = source_rows.shape
    half = width // 2
    masks = range(0, tp_count, 2)
    count = len(carried)
    if weight_rows % 128:
        normed = normalize(source_rows, gain)

        def columns(parity):
            return jnp.concatenate(
                [
                    lax.dynamic_slice_in_dim(
                        normed, (tp_at ^ m ^ parity) * weight_rows, weight_rows, 1
                    )
                    for m in masks
                ],
                axis=1,
            )

        return columns(0), columns(1), *carried

    def kernel(at_ref, rows_far, gain_far, *refs):
        far_refs, (own_ref, other_ref), near_refs = refs[:count], refs[count : count + 2], refs[count + 2 : -3]
        rows_ref, gain_ref, done = refs[-3:]
        pairs = [(rows_far, rows_ref), (gain_far, gain_ref), *zip(far_refs, near_refs)]
        copies = [
            pltpu.make_async_copy(source, target, done.at[at])
            for at, (source, target) in enumerate(pairs)
        ]
        for copy in copies:
            copy.start()
        copies[0].wait()
        copies[1].wait()
        widened = rows_ref[...].astype(F32)
        factor = lax.rsqrt(jnp.mean(widened * widened, axis=-1, keepdims=True) + EPSILON)
        for parity, out_ref in ((0, own_ref), (1, other_ref)):
            for place, m in enumerate(masks):
                start = pl.multiple_of((at_ref[0] ^ (m + parity)) * weight_rows, 128)
                at = pl.ds(start, weight_rows)
                piece = rows_ref[:, at].astype(F32) * factor * gain_ref[:, at]
                out_ref[:, place * weight_rows : (place + 1) * weight_rows] = piece.astype(BF16)
        for copy in copies[2:]:
            copy.wait()

    outs = (shape_of((rows, half), BF16), shape_of((rows, half), BF16))
    outs += tuple(shape_of(array.shape, array.dtype) for array in carried)
    return resident(
        kernel,
        outs,
        source_rows,
        gain[None],
        *carried,
        scalar=tp_at,
        far=2 + count,
        scratch=[
            pltpu.VMEM((rows, width), BF16),
            pltpu.VMEM((1, width), F32),
            pltpu.SemaphoreType.DMA((2 + count,)),
        ],
        flops=8 * rows * width,
    )


def project_some(own, other, places, weights):
    rows = own.shape[0]
    weight_rows, kv_width = weights[0][0].shape
    counts = [len(kind) for kind in weights]
    flat = [block for kind in weights for block in kind]

    def kernel(own_ref, other_ref, *refs):
        block_refs, out_refs = refs[: len(flat)], refs[len(flat) :]
        lhs = jnp.concatenate([own_ref[...], other_ref[...]], axis=0)
        for kind, out_ref in enumerate(out_refs):
            start = sum(counts[:kind])
            total = None
            for place, ref in zip(places[kind], block_refs[start : start + counts[kind]]):
                term = dot(lhs[:, place * weight_rows : (place + 1) * weight_rows], ref[...])
                total = term if total is None else total + term
            out_ref[...] = total

    outs = (shape_of((2 * rows, kv_width), F32),) * 2
    flops = 4 * rows * len(flat) * weight_rows * kv_width
    return resident(kernel, outs, own, other, *flat, flops=flops)


def project_rest(own, other, places, early, weights):
    rows = own.shape[0]
    weight_rows, kv_width = weights[0][0].shape
    counts = [len(kind) for kind in weights]
    flat = [block for kind in weights for block in kind]

    def kernel(own_ref, other_ref, *refs):
        early_refs, block_refs, (near_ref, far_ref) = refs[:2], refs[2:-2], refs[-2:]
        lhs = jnp.concatenate([own_ref[...], other_ref[...]], axis=0)
        sums = []
        for kind in range(2):
            total = early_refs[kind][...]
            start = sum(counts[:kind])
            for place, ref in zip(places[kind], block_refs[start : start + counts[kind]]):
                columns = lhs[:, place * weight_rows : (place + 1) * weight_rows]
                total = total + dot(columns, ref[...])
            sums.append(total)
        for head in range(KV_HEADS):
            at = slice(head * HEAD_DIM, (head + 1) * HEAD_DIM)
            packed = jnp.concatenate([sums[0][:, at], sums[1][:, at]], axis=1)
            near_ref[head] = packed[:rows]
            far_ref[head] = packed[rows:]

    outs = (
        shape_of((KV_HEADS, rows, 2 * HEAD_DIM), F32),
        shape_of((KV_HEADS, rows, 2 * HEAD_DIM), F32),
    )
    return resident(
        kernel, outs, own, other, *early, *flat, flops=4 * rows * len(flat) * weight_rows * kv_width
    )


def stack(arrays, lead=()):
    lead = lead or (len(arrays),)

    def kernel(*refs):
        for at, ref in enumerate(refs[:-1]):
            place = (at // lead[1], at % lead[1]) if len(lead) == 2 else (at,)
            refs[-1][place] = ref[...]

    out = shape_of((*lead, *arrays[0].shape), arrays[0].dtype)
    return resident(kernel, out, *arrays, kept=0, loaded=len(arrays))


def add_parts(own, theirs):
    def kernel(own_ref, theirs_ref, out_ref):
        out_ref[...] = (own_ref[...] + theirs_ref[...]).astype(BF16)

    return resident(kernel, shape_of(own.shape, BF16), own, theirs)


def pack_target(target_rows, cotangent, gain):
    def kernel(rows_far, gain_far, cot_far, out_ref, rows_ref, gain_ref, done):
        pairs = ((rows_far, rows_ref), (gain_far, gain_ref), (cot_far, out_ref.at[1]))
        copies = [
            pltpu.make_async_copy(source, target, done.at[at])
            for at, (source, target) in enumerate(pairs)
        ]
        for copy in copies:
            copy.start()
        copies[0].wait()
        copies[1].wait()
        out_ref[0] = normalize(rows_ref[...], gain_ref[...])
        copies[2].wait()

    return resident(
        kernel,
        shape_of((2, *target_rows.shape), BF16),
        target_rows,
        gain[None],
        cotangent,
        far=3,
        scratch=[
            pltpu.VMEM(target_rows.shape, BF16),
            pltpu.VMEM((1, target_rows.shape[1]), F32),
            pltpu.SemaphoreType.DMA((3,)),
        ],
    )


def project_target(pieces, query_weight, out_weight):
    count = sum(piece.shape[1] for piece in pieces)
    heads = query_weight.shape[1] // HEAD_DIM

    def kernel(*refs):
        piece_refs, (query_ref, weight_ref, out_ref, cot_ref) = refs[:-4], refs[-4:]
        rows = jnp.concatenate([ref[0] for ref in piece_refs], axis=0)
        queries = stacked(transposed(dot(rows, query_ref[...]))).astype(BF16)
        out_ref[0:HEAD_DIM, :] = queries * jnp.asarray(SCALE, BF16)
        cot = jnp.concatenate([ref[1] for ref in piece_refs], axis=0)
        cot_ref[...] = cot
        out_ref[HEAD_DIM:, :] = stacked(nt_dot(weight_ref[...], cot)).astype(BF16)

    out = (
        shape_of((2 * HEAD_DIM, heads * count), BF16),
        shape_of((count, pieces[0].shape[2]), BF16),
    )
    flops = 4 * count * query_weight.size
    return resident(kernel, out, *pieces, query_weight, out_weight, kept=0, flops=flops)


def gather_cotangents(pieces):
    blocks, piece_rows, width = pieces[0].shape
    count = piece_rows * len(pieces)

    def kernel(*refs):
        piece_refs, out_ref = (refs[-2], *refs[:-2]), refs[-1]
        for block in range(blocks):
            rows = jnp.concatenate([ref[block] for ref in piece_refs], axis=0)
            out_ref[block * count : (block + 1) * count, :] = rows

    out = shape_of((blocks * count, width), BF16)
    return resident(kernel, out, *pieces[1:], pieces[0], kept=0, fetched=1)


def forward_all(pairs, kv):
    blocks = len(pairs)
    lanes = pairs[0].shape[1]
    rows = kv.shape[0]
    chunk = chunk_for(rows)

    def kernel(*refs):
        pair_refs, kv_ref = refs[:blocks], refs[blocks]
        out_ref, stat_ref, *score_refs = refs[blocks + 1 :]
        zeros = jnp.zeros((HEAD_DIM, lanes), BF16)
        for block, pair_ref in enumerate(pair_refs):
            query = jnp.concatenate([pair_ref[0:HEAD_DIM, :], zeros], axis=0)
            score_ref = score_refs[block]
            peak = jnp.full((8, lanes), -jnp.inf, F32)
            for start in range(0, rows, chunk):
                scores = dot(kv_ref[start : start + chunk, :], query)
                score_ref[start : start + chunk, :] = scores
                peak = jnp.maximum(peak, jnp.max(scores.reshape(chunk // 8, 8, lanes), axis=0))
            row_max = jnp.max(peak, axis=0, keepdims=True)
            total = jnp.zeros((8, lanes), F32)
            summed = jnp.zeros((HEAD_DIM, lanes), F32)
            for start in range(0, rows, chunk):
                weights = jnp.exp(score_ref[start : start + chunk, :] - row_max)
                total = total + jnp.sum(weights.reshape(chunk // 8, 8, lanes), axis=0)
                values = kv_ref[start : start + chunk, HEAD_DIM:]
                summed = summed + tn_dot(values, weights.astype(BF16))
            total = jnp.sum(total, axis=0, keepdims=True)
            part = summed / total
            out_ref[block] = part
            stat_ref[2 * block : 2 * block + 1, :] = row_max + jnp.log(total)
            stat_ref[2 * block + 1 : 2 * block + 2, :] = jnp.sum(
                pair_ref[HEAD_DIM:, :].astype(F32) * part, axis=0, keepdims=True
            )

    outs = (shape_of((blocks, HEAD_DIM, lanes), F32), shape_of((2 * blocks, lanes), F32))
    outs += (shape_of((rows, lanes), F32),) * blocks
    return resident(
        kernel,
        outs,
        *pairs,
        kv,
        room=ROOM,
        flops=8 * blocks * rows * lanes * HEAD_DIM,
        exps=blocks * rows * lanes,
    )


def combine_stats(stats, parts):
    blocks, _, lanes = parts.shape

    def kernel(*refs):
        stat_refs, part_ref = refs[:blocks], refs[blocks]
        out_ref, *share_refs = refs[blocks + 1 :]
        for block in range(blocks):
            logs, deltas = [], []
            for peer, stat_ref in enumerate(stat_refs):
                at = 2 * (block ^ peer)
                logs.append(stat_ref[at : at + 1, :])
                deltas.append(stat_ref[at + 1 : at + 2, :])
            peak = logs[0]
            for log in logs[1:]:
                peak = jnp.maximum(peak, log)
            shares = [jnp.exp(log - peak) for log in logs]
            total = shares[0]
            delta = shares[0] * deltas[0]
            for share, term in zip(shares[1:], deltas[1:]):
                total = total + share
                delta = delta + share * term
            out_ref[2 * block : 2 * block + 1, :] = peak + jnp.log(total)
            out_ref[2 * block + 1 : 2 * block + 2, :] = delta / total
            share_refs[block][...] = (part_ref[block] * (shares[0] / total)).astype(BF16)

    outs = (shape_of((2 * blocks, lanes), F32),)
    outs += (shape_of((HEAD_DIM, lanes), BF16),) * blocks
    return resident(kernel, outs, *stats, parts, kept=1)


def backward_some(order, pairs, scores, stats, kv, sums, slots):
    count = len(order)
    lanes = pairs[0].shape[1]
    rows = kv.shape[0]
    chunk = chunk_for(rows)
    started = [] if sums is None else [sums]

    def kernel(*refs):
        pair_refs, score_refs = refs[:count], refs[count : 2 * count]
        stat_ref, kv_ref = refs[2 * count : 2 * count + 2]
        start_refs = refs[2 * count + 2 : 2 * count + 2 + len(started)]
        outs = refs[2 * count + 2 + len(started) : -1]
        sum_ref = refs[-1]
        zeros = jnp.zeros((HEAD_DIM, lanes), BF16)
        for place, block in enumerate(order):
            query = jnp.concatenate([pair_refs[place][0:HEAD_DIM, :], zeros], axis=0)
            grad = jnp.concatenate([zeros, pair_refs[place][HEAD_DIM:, :]], axis=0)
            log_total = stat_ref[2 * block : 2 * block + 1, :]
            delta = stat_ref[2 * block + 1 : 2 * block + 2, :]
            d_query = jnp.zeros((HEAD_DIM, lanes), F32)
            for start in range(0, rows, chunk):
                at = slice(start, start + chunk)
                pair = kv_ref[at, :]
                probs = jnp.exp(score_refs[place][at, :] - log_total)
                d_scores = (probs * (dot(pair, grad) - delta)).astype(BF16)
                terms = nt_dot(d_scores, query) + nt_dot(probs.astype(BF16), grad)
                if place:
                    terms = terms + sum_ref[at, :]
                elif started:
                    terms = terms + start_refs[0][at, :]
                sum_ref[at, :] = terms
                d_query = d_query + tn_dot(pair[:, :HEAD_DIM], d_scores)
            outs[1 + place][...] = (d_query * SCALE).astype(BF16)
        outs[0][...] = sum_ref[...].astype(outs[0].dtype).reshape(outs[0].shape)

    if slots:
        sum_shape = shape_of((slots, rows // slots, 2 * HEAD_DIM), BF16)
    else:
        sum_shape = shape_of((rows, 2 * HEAD_DIM), F32)
    outs = resident(
        kernel,
        (sum_shape,) + (shape_of((HEAD_DIM, lanes), BF16),) * count,
        *[pairs[block] for block in order],
        *[scores[block] for block in order],
        stats,
        kv,
        *started,
        kept=0 if slots else 1,
        scratch=[pltpu.VMEM((rows, 2 * HEAD_DIM), F32)],
        flops=20 * count * rows * lanes * HEAD_DIM,
        exps=count * rows * lanes,
    )
    return outs[1:], outs[0]


def query_back(parts, query_weight, heads):
    width = query_weight.shape[0]
    count = parts[0].shape[1] // heads
    half = count // 2

    def kernel(*refs):
        part_refs, (weight_ref, last_ref, own_ref, other_ref) = refs[:-4], refs[-4:]
        total = part_refs[0][...].astype(F32)
        for part_ref in (*part_refs[1:], last_ref):
            total = total + part_ref[...].astype(F32)
        grad = transposed(unstacked(total, heads)).astype(BF16)
        upstream = nt_dot(grad, weight_ref[...])
        own_ref[...] = upstream[:half]
        other_ref[...] = upstream[half:].astype(BF16)

    outs = (shape_of((half, width), F32), shape_of((half, width), BF16))
    flops = 2 * count * query_weight.size
    return resident(kernel, outs, *parts[:-1], query_weight, parts[-1], fetched=1, flops=flops)


def share_rows(own, theirs, count):
    rows, width = own.shape
    piece = rows // count

    def kernel(own_ref, theirs_ref, kept_ref, *out_refs):
        kept_ref[...] = own_ref[:piece, :] + theirs_ref[:piece, :].astype(F32)
        for place, out_ref in enumerate(out_refs):
            at = slice((place + 1) * piece, (place + 2) * piece)
            out_ref[...] = (own_ref[at, :] + theirs_ref[at, :].astype(F32)).astype(BF16)

    outs = (shape_of((piece, width), F32),) + (shape_of((piece, width), BF16),) * (count - 1)
    return resident(kernel, outs, own, theirs, kept=0)


def target_finish(kept, received, target_rows, cotangent, gain):
    def kernel(*refs):
        received_refs, (kept_ref, rows_ref, cot_ref, gain_ref, out_ref) = refs[:-5], refs[-5:]
        total = kept_ref[...]
        for ref in received_refs:
            total = total + ref[...].astype(F32)
        back = norm_back(rows_ref[...], gain_ref[...], total)
        out_ref[...] = cot_ref[...].astype(F32) + back

    out = shape_of(kept.shape, F32)
    args = (*received, kept, target_rows, cotangent, gain[None])
    return resident(kernel, out, *args, kept=0, loaded=len(args) - 4, fetched=4)


def attend_sum(parts):
    def kernel(*refs):
        out_ref = refs[-1]
        total = refs[0][...].astype(F32)
        for ref in refs[1:-1]:
            total = total + ref[...].astype(F32)
        out_ref[...] = total.astype(BF16)

    return resident(
        kernel, shape_of(parts[0].shape, BF16), *parts[1:], parts[0], loaded=len(parts) - 1, fetched=1
    )


def weight_grad(attended, cot_parts, heads):
    blocks = len(attended)
    count, width = cot_parts[0].shape
    half = count // 2
    step = 512 if width % 512 == 0 else width

    def kernel(*refs):
        attended_refs, cot_refs, (out_ref, wide_ref) = refs[:blocks], refs[blocks:-2], refs[-2:]

        @pl.when(pl.program_id(0) == 0)
        def _():
            for block, attended_ref in enumerate(attended_refs):
                part = unstacked(attended_ref[...].astype(F32), heads).astype(BF16)
                if not block:
                    wide_ref[:, 0:count] = part
                for core in range(2) if block else ():
                    start = count + (core * (blocks - 1) + block - 1) * half
                    wide_ref[:, start : start + half] = part[:, core * half : (core + 1) * half]

        rows = jnp.concatenate([ref[...] for ref in cot_refs], axis=0)
        out_ref[...] = dot(wide_ref[...], rows)

    specs = [pl.BlockSpec(attended[0].shape, lambda i: (0, 0))] * blocks
    specs += [pl.BlockSpec((part.shape[0], step), lambda i: (0, i)) for part in cot_parts]
    return pl.pallas_call(
        kernel,
        grid=(width // step,),
        in_specs=specs,
        out_specs=pl.BlockSpec((heads * HEAD_DIM, step), lambda i: (0, i)),
        out_shape=shape_of((heads * HEAD_DIM, width), F32),
        scratch_shapes=[pltpu.VMEM((heads * HEAD_DIM, blocks * count), BF16)],
        cost_estimate=pl.CostEstimate(
            flops=2 * heads * HEAD_DIM * blocks * count * width,
            bytes_accessed=2 * blocks * count * width,
            transcendentals=0,
        ),
        compiler_params=pltpu.CompilerParams(vmem_limit_bytes=ROOM),
        name="weight_grad",
    )(*attended, *[pltpu.with_memory_space_constraint(part, pltpu.HBM) for part in cot_parts])


def source_back(tp_at, back, held, others, source_rows, gain):
    rows, width = source_rows.shape
    _, count, weight_rows, _ = held.shape

    def kernel(at_ref, back_ref, held_ref, other_ref, rows_ref, gain_ref, out_ref):
        key_grad = jnp.concatenate([back_ref[h][:, :HEAD_DIM] for h in range(KV_HEADS)], axis=1)
        value_grad = jnp.concatenate([back_ref[h][:, HEAD_DIM:] for h in range(KV_HEADS)], axis=1)
        inner = jnp.zeros((rows, 1), F32)
        square = jnp.zeros((rows, 1), F32)
        for place in range(count):
            for parity in (0, 1):
                from_ref = other_ref if parity else held_ref
                key, value = from_ref[0, place], from_ref[1, place]
                start = pl.multiple_of((at_ref[0] ^ (2 * place + parity)) * weight_rows, 128)
                at = pl.ds(start, weight_rows)
                upstream = nt_dot(key_grad, key) + nt_dot(value_grad, value)
                weighted = upstream * gain_ref[:, at]
                widened = rows_ref[:, at].astype(F32)
                inner = inner + jnp.sum(weighted * widened, axis=-1, keepdims=True)
                square = square + jnp.sum(widened * widened, axis=-1, keepdims=True)
                out_ref[:, at] = weighted
        factor = lax.rsqrt(square / width + EPSILON)
        pull = factor**3 * (inner / width)
        out_ref[...] = factor * out_ref[...] - rows_ref[...].astype(F32) * pull

    return resident(
        kernel,
        shape_of((rows, width), F32),
        back,
        held,
        others,
        source_rows,
        gain[None],
        scalar=tp_at,
        kept=0,
        loaded=3,
        fetched=2,
        flops=4 * rows * width * KV_HEADS * HEAD_DIM,
    )


def source_back_plain(tp_at, back, held, others, source_rows, gain):
    rows, width = source_rows.shape
    _, count, weight_rows, _ = held.shape
    fulls = []
    for kind in range(2):
        full = jnp.zeros((width, KV_HEADS * HEAD_DIM), BF16)
        for place in range(count):
            start = (tp_at ^ (2 * place)) * weight_rows
            full = lax.dynamic_update_slice_in_dim(full, held[kind, place], start, 0)
            start = (tp_at ^ (2 * place + 1)) * weight_rows
            full = lax.dynamic_update_slice_in_dim(full, others[kind, place], start, 0)
        fulls.append(full)
    turned = back.transpose(1, 0, 2)
    key_grad = turned[:, :, :HEAD_DIM].reshape(rows, KV_HEADS * HEAD_DIM)
    value_grad = turned[:, :, HEAD_DIM:].reshape(rows, KV_HEADS * HEAD_DIM)
    total = nt_dot(key_grad, fulls[0]) + nt_dot(value_grad, fulls[1])
    return norm_back(source_rows, gain, total)


def body(
    target_rows,
    source_rows,
    target_gain,
    source_gain,
    query_weight,
    key_weight,
    value_weight,
    out_weight,
    out_cotangent,
):
    tp_count = lax.axis_size("tp")
    sp_count = lax.axis_size("sp")
    tp_at = lax.axis_index("tp").astype(jnp.int32)
    own_source = source_rows.shape[0]
    weight_rows = key_weight.shape[0]
    heads = query_weight.shape[1] // HEAD_DIM
    copies = max(1, tp_count // KV_HEADS)
    chips = tp_count // 2
    chip_bits = [1 << b for b in range(1, tp_count.bit_length() - 1)]
    near, far = chip_bits[: len(chip_bits) // 2], chip_bits[len(chip_bits) // 2 :]
    chip_masks = range(0, tp_count, 2)

    packed_t = pack_target(target_rows, out_cotangent, target_gain)
    own_part, other_part, query_near, out_near = split_norm(
        tp_at, source_rows, source_gain, weight_rows, tp_count, (query_weight, out_weight)
    )

    near_rows = [packed_t if m == 0 else swap(packed_t, "tp", m) for m in chip_masks]
    far_rows = [swap(rows, "tp", 1) for rows in near_rows]
    own_pieces = near_rows + far_rows
    pair, own_cot = project_target(own_pieces, query_near, out_near)
    pairs = [pair if k == 0 else swap(pair, "sp", k) for k in range(sp_count)]

    key_found = doubling(key_weight, "tp", far + near)
    value_found = doubling(value_weight, "tp", near + far)
    key_blocks = [key_found[m] for m in chip_masks]
    value_blocks = [value_found[m] for m in chip_masks]

    other_part = swap(other_part, "tp", 1)
    places = [], []
    rest = [], []
    for place, mask in enumerate(chip_masks):
        for kind, late_bits in enumerate((near, far)):
            group = rest if any(mask & bit for bit in late_bits) else places
            group[kind].append(place)
    soon = [[key_blocks[p] for p in places[0]], [value_blocks[p] for p in places[1]]]
    early = project_some(own_part, other_part, places, soon)
    late = [[key_blocks[p] for p in rest[0]], [value_blocks[p] for p in rest[1]]]
    own_sum, other_sum = project_rest(own_part, other_part, rest, early, late)
    held = stack(key_blocks + value_blocks, (2, chips))
    other_sum = swap(other_sum, "tp", 1)
    packed = add_parts(own_sum, other_sum)
    packed = jnp.repeat(packed, copies, axis=0)
    kv = lax.all_to_all(packed, "tp", split_axis=0, concat_axis=0, tiled=True)
    kv = kv.reshape(tp_count * own_source, 2 * HEAD_DIM)

    cot_z = [swap(out_cotangent, "sp", k) for k in range(1, sp_count)]
    cot_z = stack(cot_z)
    cot_near = [cot_z if m == 0 else swap(cot_z, "tp", m) for m in chip_masks]
    near_cot = gather_cotangents(cot_near)
    cot_all = [own_cot, near_cot, swap(near_cot, "tp", 1)]

    parts, own_stats, *scores = forward_all(pairs, kv)
    stats = [own_stats if k == 0 else swap(own_stats, "sp", k) for k in range(sp_count)]
    stats, *shares = combine_stats(stats, parts)
    order = list(range(sp_count // 2, sp_count)) + list(range(sp_count // 2 - 1, -1, -1))
    first, second = order[: sp_count // 2], order[sp_count // 2 :]
    found, kv_sums = backward_some(first, pairs, scores, stats, kv, None, 0)
    query_parts = [swap(part, "sp", k) for k, part in zip(first, found)]
    found, kv_sums = backward_some(second, pairs, scores, stats, kv, kv_sums, tp_count)
    query_parts += [part if k == 0 else swap(part, "sp", k) for k, part in zip(second, found)]

    others = swap(held, "tp", 1)
    back = lax.all_to_all(
        kv_sums,
        "tp",
        split_axis=0,
        concat_axis=0,
        tiled=True,
    )
    if copies > 1:
        back = back.reshape(KV_HEADS, copies, own_source, 2 * HEAD_DIM)
        back = back.astype(F32).sum(1).astype(BF16)
    finish = source_back_plain if weight_rows % 128 else source_back
    source_grad = finish(tp_at, back, held, others, source_rows, source_gain)

    mine, theirs = query_back(query_parts, query_near, heads)
    theirs = swap(theirs, "tp", 1)
    kept, *given = share_rows(mine, theirs, chips)
    received = [swap(piece, "tp", m) for m, piece in zip(list(chip_masks)[1:], given)]
    target_grad = target_finish(kept, received, target_rows, out_cotangent, target_gain)

    attended = shares[:1] + [swap(shares[k], "sp", k) for k in range(1, sp_count)]
    attended = attend_sum(attended)
    attended = [attended if k == 0 else swap(attended, "sp", k) for k in range(sp_count)]
    out_weight_grad = weight_grad(attended, cot_all, heads)
    return (target_grad, source_grad, out_weight_grad)


def solution(mesh):
    return jax.shard_map(
        body,
        mesh=mesh,
        in_specs=(
            P(("sp", "tp"), None),
            P(("sp", "tp"), None),
            P(),
            P(),
            P(None, "tp"),
            P("tp", None),
            P("tp", None),
            P("tp", None),
            P(("sp", "tp"), None),
        ),
        out_specs=(P(("sp", "tp"), None), P(("sp", "tp"), None), P("tp", None)),
        check_vma=False,
    )
```

```python
import jax
import jax.numpy as jnp
from jax import lax
from jax.experimental import pallas as pl
from jax.experimental.pallas import tpu as pltpu
from jax.sharding import PartitionSpec as P


HEAD_DIM = 64
KV_HEADS = 8
EPSILON = 1e-06
SCALE = HEAD_DIM**-0.5


F32 = jnp.float32
BF16 = jnp.bfloat16


def shape_of(shape, dtype):
    return jax.ShapeDtypeStruct(shape, dtype)


def normalize(matrix, gain_vector):
    widened = matrix.astype(F32)
    factor = lax.rsqrt(jnp.mean(widened * widened, axis=-1, keepdims=True) + EPSILON)
    return (widened * factor * gain_vector).astype(BF16)


def norm_back(matrix, gain_vector, upstream):
    widened = matrix.astype(F32)
    factor = lax.rsqrt(jnp.mean(widened * widened, axis=-1, keepdims=True) + EPSILON)
    weighted = upstream * gain_vector
    inner_sum = jnp.mean(weighted * widened, axis=-1, keepdims=True)
    return factor * weighted - widened * factor**3 * inner_sum


def swap(array, axis, mask):
    size = lax.axis_size(axis)
    return lax.ppermute(array, axis, [(i, i ^ mask) for i in range(size)])


def doubling(array, axis, bits):
    blocks = {0: array}
    for bit in bits:
        received = {key ^ bit: swap(value, axis, bit) for key, value in blocks.items()}
        blocks.update(received)
    return blocks


def dot(a, b):
    return jnp.dot(a, b, preferred_element_type=F32)


def nt_dot(a, b):
    return lax.dot_general(a, b, (((1,), (1,)), ((), ())), preferred_element_type=F32)


def tn_dot(a, b):
    return lax.dot_general(a, b, (((0,), (0,)), ((), ())), preferred_element_type=F32)


def chunk_for(rows):
    return 256 if rows % 256 == 0 else rows


def pad_to(extent, multiple):
    return -(-extent // multiple) * multiple


def transposed(matrix):
    rows, columns = matrix.shape
    more_rows, more_columns = pad_to(rows, 128) - rows, pad_to(columns, 128) - columns
    if more_columns:
        matrix = jnp.concatenate([matrix, jnp.zeros((rows, more_columns), F32)], axis=1)
    if more_rows:
        filler = jnp.zeros((more_rows, columns + more_columns), F32)
        matrix = jnp.concatenate([matrix, filler], axis=0)
    return matrix.T[:columns, :rows]


def stacked(matrix):
    heads = matrix.shape[0] // HEAD_DIM
    pieces = [matrix[g * HEAD_DIM : (g + 1) * HEAD_DIM, :] for g in range(heads)]
    return jnp.concatenate(pieces, axis=1) if heads > 1 else pieces[0]


def unstacked(matrix, heads):
    rows = matrix.shape[1] // heads
    pieces = [matrix[:, g * rows : (g + 1) * rows] for g in range(heads)]
    return jnp.concatenate(pieces, axis=0) if heads > 1 else pieces[0]


SCALAR = pl.BlockSpec(memory_space=pltpu.SMEM)
WHOLE = pl.BlockSpec(memory_space=pltpu.VMEM)
ROOM = 16 << 20


def resident(
    kernel,
    out_shape,
    *args,
    scalar=None,
    kept=None,
    loaded=0,
    fetched=0,
    far=0,
    scratch=(),
    room=ROOM,
    **costs,
):
    single = not isinstance(out_shape, tuple)
    outs = (out_shape,) if single else out_shape
    kept = len(outs) if kept is None else kept
    outs = tuple(
        (pltpu.VMEM if at < kept else pltpu.HBM)(out.shape, out.dtype)
        for at, out in enumerate(outs)
    )
    near = len(args) - far
    specs = [WHOLE] * near + [pl.BlockSpec(memory_space=pltpu.HBM)] * far
    held = near - fetched

    def placed(at, arg):
        if at < held - loaded:
            return pltpu.with_memory_space_constraint(arg, pltpu.VMEM)
        return arg if at < held else pltpu.with_memory_space_constraint(arg, pltpu.HBM)

    args = [placed(at, arg) for at, arg in enumerate(args)]
    if scalar is not None:
        args, specs = [scalar[None]] + args, [SCALAR] + specs
    return pl.pallas_call(
        kernel,
        out_shape=outs[0] if single else outs,
        in_specs=specs,
        out_specs=WHOLE if single else (WHOLE,) * len(outs),
        scratch_shapes=list(scratch),
        cost_estimate=pl.CostEstimate(
            flops=costs.get("flops", 1 << 20),
            bytes_accessed=costs.get("moved", 1 << 20),
            transcendentals=costs.get("exps", 0),
        ),
        compiler_params=pltpu.CompilerParams(vmem_limit_bytes=room),
    )(*args)


def split_norm(tp_at, source_rows, gain, weight_rows, tp_count, carried):
    rows, width = source_rows.shape
    half = width // 2
    masks = range(0, tp_count, 2)
    count = len(carried)
    if weight_rows % 128:
        normed = normalize(source_rows, gain)

        def columns(parity):
            return jnp.concatenate(
                [
                    lax.dynamic_slice_in_dim(
                        normed, (tp_at ^ m ^ parity) * weight_rows, weight_rows, 1
                    )
                    for m in masks
                ],
                axis=1,
            )

        return columns(0), columns(1), *carried

    def kernel(at_ref, rows_far, gain_far, *refs):
        far_refs, (own_ref, other_ref), near_refs = refs[:count], refs[count : count + 2], refs[count + 2 : -3]
        rows_ref, gain_ref, done = refs[-3:]
        pairs = [(rows_far, rows_ref), (gain_far, gain_ref), *zip(far_refs, near_refs)]
        copies = [
            pltpu.make_async_copy(source, target, done.at[at])
            for at, (source, target) in enumerate(pairs)
        ]
        for copy in copies:
            copy.start()
        copies[0].wait()
        copies[1].wait()
        widened = rows_ref[...].astype(F32)
        factor = lax.rsqrt(jnp.mean(widened * widened, axis=-1, keepdims=True) + EPSILON)
        for parity, out_ref in ((0, own_ref), (1, other_ref)):
            for place, m in enumerate(masks):
                start = pl.multiple_of((at_ref[0] ^ (m + parity)) * weight_rows, 128)
                at = pl.ds(start, weight_rows)
                piece = rows_ref[:, at].astype(F32) * factor * gain_ref[:, at]
                out_ref[:, place * weight_rows : (place + 1) * weight_rows] = piece.astype(BF16)
        for copy in copies[2:]:
            copy.wait()

    outs = (shape_of((rows, half), BF16), shape_of((rows, half), BF16))
    outs += tuple(shape_of(array.shape, array.dtype) for array in carried)
    return resident(
        kernel,
        outs,
        source_rows,
        gain[None],
        *carried,
        scalar=tp_at,
        far=2 + count,
        scratch=[
            pltpu.VMEM((rows, width), BF16),
            pltpu.VMEM((1, width), F32),
            pltpu.SemaphoreType.DMA((2 + count,)),
        ],
        flops=8 * rows * width,
    )


def project_some(own, other, places, weights):
    rows = own.shape[0]
    weight_rows, kv_width = weights[0][0].shape
    counts = [len(kind) for kind in weights]
    flat = [block for kind in weights for block in kind]

    def kernel(own_ref, other_ref, *refs):
        block_refs, out_refs = refs[: len(flat)], refs[len(flat) :]
        lhs = jnp.concatenate([own_ref[...], other_ref[...]], axis=0)
        for kind, out_ref in enumerate(out_refs):
            start = sum(counts[:kind])
            total = None
            for place, ref in zip(places[kind], block_refs[start : start + counts[kind]]):
                term = dot(lhs[:, place * weight_rows : (place + 1) * weight_rows], ref[...])
                total = term if total is None else total + term
            out_ref[...] = total

    outs = (shape_of((2 * rows, kv_width), F32),) * 2
    flops = 4 * rows * len(flat) * weight_rows * kv_width
    return resident(kernel, outs, own, other, *flat, flops=flops)


def project_rest(own, other, places, early, weights):
    rows = own.shape[0]
    weight_rows, kv_width = weights[0][0].shape
    counts = [len(kind) for kind in weights]
    flat = [block for kind in weights for block in kind]

    def kernel(own_ref, other_ref, *refs):
        early_refs, block_refs, (near_ref, far_ref) = refs[:2], refs[2:-2], refs[-2:]
        lhs = jnp.concatenate([own_ref[...], other_ref[...]], axis=0)
        sums = []
        for kind in range(2):
            total = early_refs[kind][...]
            start = sum(counts[:kind])
            for place, ref in zip(places[kind], block_refs[start : start + counts[kind]]):
                columns = lhs[:, place * weight_rows : (place + 1) * weight_rows]
                total = total + dot(columns, ref[...])
            sums.append(total)
        for head in range(KV_HEADS):
            at = slice(head * HEAD_DIM, (head + 1) * HEAD_DIM)
            packed = jnp.concatenate([sums[0][:, at], sums[1][:, at]], axis=1)
            near_ref[head] = packed[:rows]
            far_ref[head] = packed[rows:]

    outs = (
        shape_of((KV_HEADS, rows, 2 * HEAD_DIM), F32),
        shape_of((KV_HEADS, rows, 2 * HEAD_DIM), F32),
    )
    return resident(
        kernel, outs, own, other, *early, *flat, flops=4 * rows * len(flat) * weight_rows * kv_width
    )


def stack(arrays, lead=()):
    lead = lead or (len(arrays),)

    def kernel(*refs):
        for at, ref in enumerate(refs[:-1]):
            place = (at // lead[1], at % lead[1]) if len(lead) == 2 else (at,)
            refs[-1][place] = ref[...]

    out = shape_of((*lead, *arrays[0].shape), arrays[0].dtype)
    return resident(kernel, out, *arrays, kept=0, loaded=len(arrays))


def add_parts(own, theirs):
    def kernel(own_ref, theirs_ref, out_ref):
        out_ref[...] = (own_ref[...] + theirs_ref[...]).astype(BF16)

    return resident(kernel, shape_of(own.shape, BF16), own, theirs)


def pack_target(target_rows, cotangent, gain):
    def kernel(rows_far, gain_far, cot_far, out_ref, rows_ref, gain_ref, done):
        pairs = ((rows_far, rows_ref), (gain_far, gain_ref), (cot_far, out_ref.at[1]))
        copies = [
            pltpu.make_async_copy(source, target, done.at[at])
            for at, (source, target) in enumerate(pairs)
        ]
        for copy in copies:
            copy.start()
        copies[0].wait()
        copies[1].wait()
        out_ref[0] = normalize(rows_ref[...], gain_ref[...])
        copies[2].wait()

    return resident(
        kernel,
        shape_of((2, *target_rows.shape), BF16),
        target_rows,
        gain[None],
        cotangent,
        far=3,
        scratch=[
            pltpu.VMEM(target_rows.shape, BF16),
            pltpu.VMEM((1, target_rows.shape[1]), F32),
            pltpu.SemaphoreType.DMA((3,)),
        ],
    )


def project_target(pieces, query_weight, out_weight):
    count = sum(piece.shape[1] for piece in pieces)
    heads = query_weight.shape[1] // HEAD_DIM

    def kernel(*refs):
        piece_refs, (query_ref, weight_ref, out_ref) = refs[:-3], refs[-3:]
        rows = jnp.concatenate([ref[0] for ref in piece_refs], axis=0)
        queries = stacked(transposed(dot(rows, query_ref[...]))).astype(BF16)
        out_ref[0:HEAD_DIM, :] = queries * jnp.asarray(SCALE, BF16)
        cot = jnp.concatenate([ref[1] for ref in piece_refs], axis=0)
        out_ref[HEAD_DIM:, :] = stacked(nt_dot(weight_ref[...], cot)).astype(BF16)

    out = shape_of((2 * HEAD_DIM, heads * count), BF16)
    flops = 4 * count * query_weight.size
    return resident(kernel, out, *pieces, query_weight, out_weight, kept=0, flops=flops)


def hold_own(pieces, pair):
    count = sum(piece.shape[1] for piece in pieces)

    def kernel(*refs):
        piece_refs, (pair_ref, near_ref, out_ref) = refs[:-3], refs[-3:]
        near_ref[...] = pair_ref[...]
        out_ref[...] = jnp.concatenate([ref[1] for ref in piece_refs], axis=0)

    outs = (shape_of(pair.shape, BF16), shape_of((count, pieces[0].shape[2]), BF16))
    return resident(kernel, outs, *pieces, pair, kept=1, loaded=len(pieces), fetched=1)


def gather_cotangents(pieces):
    blocks, piece_rows, width = pieces[0].shape
    count = piece_rows * len(pieces)

    def kernel(*refs):
        piece_refs, out_ref = (refs[-2], *refs[:-2]), refs[-1]
        for block in range(blocks):
            rows = jnp.concatenate([ref[block] for ref in piece_refs], axis=0)
            out_ref[block * count : (block + 1) * count, :] = rows

    out = shape_of((blocks * count, width), BF16)
    return resident(kernel, out, *pieces[1:], pieces[0], kept=0, fetched=1)


def forward_all(pairs, kv):
    blocks = len(pairs)
    lanes = pairs[0].shape[1]
    rows = kv.shape[0]
    chunk = chunk_for(rows)

    def kernel(*refs):
        pair_refs, kv_ref = refs[:blocks], refs[blocks]
        out_ref, stat_ref, *score_refs = refs[blocks + 1 :]
        zeros = jnp.zeros((HEAD_DIM, lanes), BF16)
        for block, pair_ref in enumerate(pair_refs):
            query = jnp.concatenate([pair_ref[0:HEAD_DIM, :], zeros], axis=0)
            score_ref = score_refs[block]
            peak = jnp.full((8, lanes), -jnp.inf, F32)
            for start in range(0, rows, chunk):
                scores = dot(kv_ref[start : start + chunk, :], query)
                score_ref[start : start + chunk, :] = scores
                peak = jnp.maximum(peak, jnp.max(scores.reshape(chunk // 8, 8, lanes), axis=0))
            row_max = jnp.max(peak, axis=0, keepdims=True)
            total = jnp.zeros((8, lanes), F32)
            summed = jnp.zeros((HEAD_DIM, lanes), F32)
            for start in range(0, rows, chunk):
                weights = jnp.exp(score_ref[start : start + chunk, :] - row_max)
                total = total + jnp.sum(weights.reshape(chunk // 8, 8, lanes), axis=0)
                values = kv_ref[start : start + chunk, HEAD_DIM:]
                summed = summed + tn_dot(values, weights.astype(BF16))
            total = jnp.sum(total, axis=0, keepdims=True)
            part = summed / total
            out_ref[block] = part
            stat_ref[2 * block : 2 * block + 1, :] = row_max + jnp.log(total)
            stat_ref[2 * block + 1 : 2 * block + 2, :] = jnp.sum(
                pair_ref[HEAD_DIM:, :].astype(F32) * part, axis=0, keepdims=True
            )

    outs = (shape_of((blocks, HEAD_DIM, lanes), F32), shape_of((2 * blocks, lanes), F32))
    outs += (shape_of((rows, lanes), F32),) * blocks
    return resident(
        kernel,
        outs,
        *pairs,
        kv,
        room=ROOM,
        flops=8 * blocks * rows * lanes * HEAD_DIM,
        exps=blocks * rows * lanes,
    )


def combine_stats(stats, parts):
    blocks, _, lanes = parts.shape

    def kernel(*refs):
        stat_refs, part_ref = refs[:blocks], refs[blocks]
        out_ref, *share_refs = refs[blocks + 1 :]
        for block in range(blocks):
            logs, deltas = [], []
            for peer, stat_ref in enumerate(stat_refs):
                at = 2 * (block ^ peer)
                logs.append(stat_ref[at : at + 1, :])
                deltas.append(stat_ref[at + 1 : at + 2, :])
            peak = logs[0]
            for log in logs[1:]:
                peak = jnp.maximum(peak, log)
            shares = [jnp.exp(log - peak) for log in logs]
            total = shares[0]
            delta = shares[0] * deltas[0]
            for share, term in zip(shares[1:], deltas[1:]):
                total = total + share
                delta = delta + share * term
            out_ref[2 * block : 2 * block + 1, :] = peak + jnp.log(total)
            out_ref[2 * block + 1 : 2 * block + 2, :] = delta / total
            share_refs[block][...] = (part_ref[block] * (shares[0] / total)).astype(BF16)

    outs = (shape_of((2 * blocks, lanes), F32),)
    outs += (shape_of((HEAD_DIM, lanes), BF16),) * blocks
    return resident(kernel, outs, *stats, parts, kept=1)


def backward_some(order, pairs, scores, stats, kv, sums, slots):
    count = len(order)
    lanes = pairs[0].shape[1]
    rows = kv.shape[0]
    chunk = chunk_for(rows)
    started = [] if sums is None else [sums]

    def kernel(*refs):
        pair_refs, score_refs = refs[:count], refs[count : 2 * count]
        stat_ref, kv_ref = refs[2 * count : 2 * count + 2]
        start_refs = refs[2 * count + 2 : 2 * count + 2 + len(started)]
        outs = refs[2 * count + 2 + len(started) : -1]
        sum_ref = refs[-1]
        zeros = jnp.zeros((HEAD_DIM, lanes), BF16)
        for place, block in enumerate(order):
            query = jnp.concatenate([pair_refs[place][0:HEAD_DIM, :], zeros], axis=0)
            grad = jnp.concatenate([zeros, pair_refs[place][HEAD_DIM:, :]], axis=0)
            log_total = stat_ref[2 * block : 2 * block + 1, :]
            delta = stat_ref[2 * block + 1 : 2 * block + 2, :]
            d_query = jnp.zeros((HEAD_DIM, lanes), F32)
            for start in range(0, rows, chunk):
                at = slice(start, start + chunk)
                pair = kv_ref[at, :]
                probs = jnp.exp(score_refs[place][at, :] - log_total)
                d_scores = (probs * (dot(pair, grad) - delta)).astype(BF16)
                terms = nt_dot(d_scores, query) + nt_dot(probs.astype(BF16), grad)
                if place:
                    terms = terms + sum_ref[at, :]
                elif started:
                    terms = terms + start_refs[0][at, :]
                sum_ref[at, :] = terms
                d_query = d_query + tn_dot(pair[:, :HEAD_DIM], d_scores)
            outs[1 + place][...] = (d_query * SCALE).astype(BF16)
        outs[0][...] = sum_ref[...].astype(outs[0].dtype).reshape(outs[0].shape)

    if slots:
        sum_shape = shape_of((slots, rows // slots, 2 * HEAD_DIM), BF16)
    else:
        sum_shape = shape_of((rows, 2 * HEAD_DIM), F32)
    outs = resident(
        kernel,
        (sum_shape,) + (shape_of((HEAD_DIM, lanes), BF16),) * count,
        *[pairs[block] for block in order],
        *[scores[block] for block in order],
        stats,
        kv,
        *started,
        kept=0 if slots else 1,
        scratch=[pltpu.VMEM((rows, 2 * HEAD_DIM), F32)],
        flops=20 * count * rows * lanes * HEAD_DIM,
        exps=count * rows * lanes,
    )
    return outs[1:], outs[0]


def query_back(parts, query_weight, heads):
    width = query_weight.shape[0]
    count = parts[0].shape[1] // heads
    half = count // 2

    def kernel(*refs):
        part_refs, (weight_ref, last_ref, own_ref, other_ref) = refs[:-4], refs[-4:]
        total = part_refs[0][...].astype(F32)
        for part_ref in (*part_refs[1:], last_ref):
            total = total + part_ref[...].astype(F32)
        grad = transposed(unstacked(total, heads)).astype(BF16)
        upstream = nt_dot(grad, weight_ref[...])
        own_ref[...] = upstream[:half]
        other_ref[...] = upstream[half:].astype(BF16)

    outs = (shape_of((half, width), F32), shape_of((half, width), BF16))
    flops = 2 * count * query_weight.size
    return resident(kernel, outs, *parts[:-1], query_weight, parts[-1], fetched=1, flops=flops)


def share_rows(own, theirs, count):
    rows, width = own.shape
    piece = rows // count

    def kernel(own_ref, theirs_ref, kept_ref, *out_refs):
        kept_ref[...] = own_ref[:piece, :] + theirs_ref[:piece, :].astype(F32)
        for place, out_ref in enumerate(out_refs):
            at = slice((place + 1) * piece, (place + 2) * piece)
            out_ref[...] = (own_ref[at, :] + theirs_ref[at, :].astype(F32)).astype(BF16)

    outs = (shape_of((piece, width), F32),) + (shape_of((piece, width), BF16),) * (count - 1)
    return resident(kernel, outs, own, theirs, kept=0)


def target_finish(kept, received, target_rows, cotangent, gain):
    def kernel(*refs):
        received_refs, (kept_ref, rows_ref, cot_ref, gain_ref, out_ref) = refs[:-5], refs[-5:]
        total = kept_ref[...]
        for ref in received_refs:
            total = total + ref[...].astype(F32)
        back = norm_back(rows_ref[...], gain_ref[...], total)
        out_ref[...] = cot_ref[...].astype(F32) + back

    out = shape_of(kept.shape, F32)
    args = (*received, kept, target_rows, cotangent, gain[None])
    return resident(kernel, out, *args, kept=0, loaded=len(args) - 4, fetched=4)


def attend_sum(parts):
    def kernel(*refs):
        out_ref = refs[-1]
        total = refs[0][...].astype(F32)
        for ref in refs[1:-1]:
            total = total + ref[...].astype(F32)
        out_ref[...] = total.astype(BF16)

    return resident(
        kernel, shape_of(parts[0].shape, BF16), *parts[1:], parts[0], loaded=len(parts) - 1, fetched=1
    )


def weight_grad(attended, cot_parts, heads):
    blocks = len(attended)
    count, width = cot_parts[0].shape
    half = count // 2
    step = 1024 if width % 1024 == 0 else width

    def kernel(*refs):
        attended_refs, cot_refs, (out_ref, wide_ref) = refs[:blocks], refs[blocks:-2], refs[-2:]

        @pl.when(pl.program_id(0) == 0)
        def _():
            for block, attended_ref in enumerate(attended_refs):
                part = unstacked(attended_ref[...].astype(F32), heads).astype(BF16)
                if not block:
                    wide_ref[:, 0:count] = part
                for core in range(2) if block else ():
                    start = count + (core * (blocks - 1) + block - 1) * half
                    wide_ref[:, start : start + half] = part[:, core * half : (core + 1) * half]

        rows = jnp.concatenate([ref[...] for ref in cot_refs], axis=0)
        out_ref[...] = dot(wide_ref[...], rows)

    specs = [pl.BlockSpec(attended[0].shape, lambda i: (0, 0))] * blocks
    specs += [pl.BlockSpec((part.shape[0], step), lambda i: (0, i)) for part in cot_parts]
    return pl.pallas_call(
        kernel,
        grid=(width // step,),
        in_specs=specs,
        out_specs=pl.BlockSpec((heads * HEAD_DIM, step), lambda i: (0, i)),
        out_shape=shape_of((heads * HEAD_DIM, width), F32),
        scratch_shapes=[pltpu.VMEM((heads * HEAD_DIM, blocks * count), BF16)],
        cost_estimate=pl.CostEstimate(
            flops=2 * heads * HEAD_DIM * blocks * count * width,
            bytes_accessed=2 * blocks * count * width,
            transcendentals=0,
        ),
        compiler_params=pltpu.CompilerParams(vmem_limit_bytes=ROOM),
        name="weight_grad",
    )(*attended, *[pltpu.with_memory_space_constraint(part, pltpu.HBM) for part in cot_parts])


def source_back(tp_at, back, held, others, source_rows, gain):
    rows, width = source_rows.shape
    _, count, weight_rows, _ = held.shape

    def kernel(at_ref, back_ref, held_ref, other_ref, rows_ref, gain_ref, out_ref):
        key_grad = jnp.concatenate([back_ref[h][:, :HEAD_DIM] for h in range(KV_HEADS)], axis=1)
        value_grad = jnp.concatenate([back_ref[h][:, HEAD_DIM:] for h in range(KV_HEADS)], axis=1)
        inner = jnp.zeros((rows, 1), F32)
        square = jnp.zeros((rows, 1), F32)
        for place in range(count):
            for parity in (0, 1):
                from_ref = other_ref if parity else held_ref
                key, value = from_ref[0, place], from_ref[1, place]
                start = pl.multiple_of((at_ref[0] ^ (2 * place + parity)) * weight_rows, 128)
                at = pl.ds(start, weight_rows)
                upstream = nt_dot(key_grad, key) + nt_dot(value_grad, value)
                weighted = upstream * gain_ref[:, at]
                widened = rows_ref[:, at].astype(F32)
                inner = inner + jnp.sum(weighted * widened, axis=-1, keepdims=True)
                square = square + jnp.sum(widened * widened, axis=-1, keepdims=True)
                out_ref[:, at] = weighted
        factor = lax.rsqrt(square / width + EPSILON)
        pull = factor**3 * (inner / width)
        out_ref[...] = factor * out_ref[...] - rows_ref[...].astype(F32) * pull

    return resident(
        kernel,
        shape_of((rows, width), F32),
        back,
        held,
        others,
        source_rows,
        gain[None],
        scalar=tp_at,
        kept=0,
        loaded=3,
        fetched=2,
        flops=4 * rows * width * KV_HEADS * HEAD_DIM,
    )


def source_back_plain(tp_at, back, held, others, source_rows, gain):
    rows, width = source_rows.shape
    _, count, weight_rows, _ = held.shape
    fulls = []
    for kind in range(2):
        full = jnp.zeros((width, KV_HEADS * HEAD_DIM), BF16)
        for place in range(count):
            start = (tp_at ^ (2 * place)) * weight_rows
            full = lax.dynamic_update_slice_in_dim(full, held[kind, place], start, 0)
            start = (tp_at ^ (2 * place + 1)) * weight_rows
            full = lax.dynamic_update_slice_in_dim(full, others[kind, place], start, 0)
        fulls.append(full)
    turned = back.transpose(1, 0, 2)
    key_grad = turned[:, :, :HEAD_DIM].reshape(rows, KV_HEADS * HEAD_DIM)
    value_grad = turned[:, :, HEAD_DIM:].reshape(rows, KV_HEADS * HEAD_DIM)
    total = nt_dot(key_grad, fulls[0]) + nt_dot(value_grad, fulls[1])
    return norm_back(source_rows, gain, total)


def body(
    target_rows,
    source_rows,
    target_gain,
    source_gain,
    query_weight,
    key_weight,
    value_weight,
    out_weight,
    out_cotangent,
):
    tp_count = lax.axis_size("tp")
    sp_count = lax.axis_size("sp")
    tp_at = lax.axis_index("tp").astype(jnp.int32)
    own_source = source_rows.shape[0]
    weight_rows = key_weight.shape[0]
    heads = query_weight.shape[1] // HEAD_DIM
    copies = max(1, tp_count // KV_HEADS)
    chips = tp_count // 2
    chip_bits = [1 << b for b in range(1, tp_count.bit_length() - 1)]
    near, far = chip_bits[: len(chip_bits) // 2], chip_bits[len(chip_bits) // 2 :]
    chip_masks = range(0, tp_count, 2)

    packed_t = pack_target(target_rows, out_cotangent, target_gain)
    own_part, other_part, query_near, out_near = split_norm(
        tp_at, source_rows, source_gain, weight_rows, tp_count, (query_weight, out_weight)
    )

    near_rows = [packed_t if m == 0 else swap(packed_t, "tp", m) for m in chip_masks]
    far_rows = [swap(rows, "tp", 1) for rows in near_rows]
    own_pieces = near_rows + far_rows
    pair = project_target(own_pieces, query_near, out_near)
    pair_near, own_cot = hold_own(own_pieces, pair)
    pairs = [pair if k == 0 else swap(pair, "sp", k) for k in range(sp_count)]

    key_found = doubling(key_weight, "tp", far + near)
    value_found = doubling(value_weight, "tp", near + far)
    key_blocks = [key_found[m] for m in chip_masks]
    value_blocks = [value_found[m] for m in chip_masks]

    other_part = swap(other_part, "tp", 1)
    places = [], []
    rest = [], []
    for place, mask in enumerate(chip_masks):
        for kind, late_bits in enumerate((near, far)):
            group = rest if any(mask & bit for bit in late_bits) else places
            group[kind].append(place)
    soon = [[key_blocks[p] for p in places[0]], [value_blocks[p] for p in places[1]]]
    early = project_some(own_part, other_part, places, soon)
    late = [[key_blocks[p] for p in rest[0]], [value_blocks[p] for p in rest[1]]]
    own_sum, other_sum = project_rest(own_part, other_part, rest, early, late)
    held = stack(key_blocks + value_blocks, (2, chips))
    other_sum = swap(other_sum, "tp", 1)
    packed = add_parts(own_sum, other_sum)
    packed = jnp.repeat(packed, copies, axis=0)
    kv = lax.all_to_all(packed, "tp", split_axis=0, concat_axis=0, tiled=True)
    kv = kv.reshape(tp_count * own_source, 2 * HEAD_DIM)

    cot_z = [swap(out_cotangent, "sp", k) for k in range(1, sp_count)]
    cot_z = stack(cot_z)
    cot_near = [cot_z if m == 0 else swap(cot_z, "tp", m) for m in chip_masks]
    near_cot = gather_cotangents(cot_near)
    cot_all = [own_cot, near_cot, swap(near_cot, "tp", 1)]

    parts, own_stats, *scores = forward_all([pair_near] + pairs[1:], kv)
    stats = [own_stats if k == 0 else swap(own_stats, "sp", k) for k in range(sp_count)]
    stats, *shares = combine_stats(stats, parts)
    order = list(range(sp_count // 2, sp_count)) + list(range(sp_count // 2 - 1, -1, -1))
    first, second = order[: sp_count // 2], order[sp_count // 2 :]
    found, kv_sums = backward_some(first, pairs, scores, stats, kv, None, 0)
    query_parts = [swap(part, "sp", k) for k, part in zip(first, found)]
    found, kv_sums = backward_some(second, pairs, scores, stats, kv, kv_sums, tp_count)
    query_parts += [part if k == 0 else swap(part, "sp", k) for k, part in zip(second, found)]

    others = swap(held, "tp", 1)
    back = lax.all_to_all(
        kv_sums,
        "tp",
        split_axis=0,
        concat_axis=0,
        tiled=True,
    )
    if copies > 1:
        back = back.reshape(KV_HEADS, copies, own_source, 2 * HEAD_DIM)
        back = back.astype(F32).sum(1).astype(BF16)
    finish = source_back_plain if weight_rows % 128 else source_back
    source_grad = finish(tp_at, back, held, others, source_rows, source_gain)

    mine, theirs = query_back(query_parts, query_near, heads)
    theirs = swap(theirs, "tp", 1)
    kept, *given = share_rows(mine, theirs, chips)
    received = [swap(piece, "tp", m) for m, piece in zip(list(chip_masks)[1:], given)]
    target_grad = target_finish(kept, received, target_rows, out_cotangent, target_gain)

    attended = shares[:1] + [swap(shares[k], "sp", k) for k in range(1, sp_count)]
    attended = attend_sum(attended)
    attended = [attended if k == 0 else swap(attended, "sp", k) for k in range(sp_count)]
    out_weight_grad = weight_grad(attended, cot_all, heads)
    return (target_grad, source_grad, out_weight_grad)


def solution(mesh):
    return jax.shard_map(
        body,
        mesh=mesh,
        in_specs=(
            P(("sp", "tp"), None),
            P(("sp", "tp"), None),
            P(),
            P(),
            P(None, "tp"),
            P("tp", None),
            P("tp", None),
            P("tp", None),
            P(("sp", "tp"), None),
        ),
        out_specs=(P(("sp", "tp"), None), P(("sp", "tp"), None), P("tp", None)),
        check_vma=False,
    )
```

```python
import jax
import jax.numpy as jnp
from jax import lax
from jax.experimental import pallas as pl
from jax.experimental.pallas import tpu as pltpu
from jax.sharding import PartitionSpec as P


HEAD_DIM = 64
KV_HEADS = 8
EPSILON = 1e-06
SCALE = HEAD_DIM**-0.5


F32 = jnp.float32
BF16 = jnp.bfloat16


def shape_of(shape, dtype):
    return jax.ShapeDtypeStruct(shape, dtype)


def normalize(matrix, gain_vector):
    widened = matrix.astype(F32)
    factor = lax.rsqrt(jnp.mean(widened * widened, axis=-1, keepdims=True) + EPSILON)
    return (widened * factor * gain_vector).astype(BF16)


def norm_back(matrix, gain_vector, upstream):
    widened = matrix.astype(F32)
    factor = lax.rsqrt(jnp.mean(widened * widened, axis=-1, keepdims=True) + EPSILON)
    weighted = upstream * gain_vector
    inner_sum = jnp.mean(weighted * widened, axis=-1, keepdims=True)
    return factor * weighted - widened * factor**3 * inner_sum


def swap(array, axis, mask):
    size = lax.axis_size(axis)
    return lax.ppermute(array, axis, [(i, i ^ mask) for i in range(size)])


def doubling(array, axis, bits):
    blocks = {0: array}
    for bit in bits:
        received = {key ^ bit: swap(value, axis, bit) for key, value in blocks.items()}
        blocks.update(received)
    return blocks


def dot(a, b):
    return jnp.dot(a, b, preferred_element_type=F32)


def nt_dot(a, b):
    return lax.dot_general(a, b, (((1,), (1,)), ((), ())), preferred_element_type=F32)


def tn_dot(a, b):
    return lax.dot_general(a, b, (((0,), (0,)), ((), ())), preferred_element_type=F32)


def chunk_for(rows):
    return 256 if rows % 256 == 0 else rows


def pad_to(extent, multiple):
    return -(-extent // multiple) * multiple


def transposed(matrix):
    rows, columns = matrix.shape
    more_rows, more_columns = pad_to(rows, 128) - rows, pad_to(columns, 128) - columns
    if more_columns:
        matrix = jnp.concatenate([matrix, jnp.zeros((rows, more_columns), F32)], axis=1)
    if more_rows:
        filler = jnp.zeros((more_rows, columns + more_columns), F32)
        matrix = jnp.concatenate([matrix, filler], axis=0)
    return matrix.T[:columns, :rows]


def stacked(matrix):
    heads = matrix.shape[0] // HEAD_DIM
    pieces = [matrix[g * HEAD_DIM : (g + 1) * HEAD_DIM, :] for g in range(heads)]
    return jnp.concatenate(pieces, axis=1) if heads > 1 else pieces[0]


def unstacked(matrix, heads):
    rows = matrix.shape[1] // heads
    pieces = [matrix[:, g * rows : (g + 1) * rows] for g in range(heads)]
    return jnp.concatenate(pieces, axis=0) if heads > 1 else pieces[0]


SCALAR = pl.BlockSpec(memory_space=pltpu.SMEM)
WHOLE = pl.BlockSpec(memory_space=pltpu.VMEM)
ROOM = 16 << 20


def resident(
    kernel,
    out_shape,
    *args,
    scalar=None,
    kept=None,
    loaded=0,
    fetched=0,
    far=0,
    scratch=(),
    room=ROOM,
    **costs,
):
    single = not isinstance(out_shape, tuple)
    outs = (out_shape,) if single else out_shape
    kept = len(outs) if kept is None else kept
    outs = tuple(
        (pltpu.VMEM if at < kept else pltpu.HBM)(out.shape, out.dtype)
        for at, out in enumerate(outs)
    )
    near = len(args) - far
    specs = [WHOLE] * near + [pl.BlockSpec(memory_space=pltpu.HBM)] * far
    held = near - fetched

    def placed(at, arg):
        if at < held - loaded:
            return pltpu.with_memory_space_constraint(arg, pltpu.VMEM)
        return arg if at < held else pltpu.with_memory_space_constraint(arg, pltpu.HBM)

    args = [placed(at, arg) for at, arg in enumerate(args)]
    if scalar is not None:
        args, specs = [scalar[None]] + args, [SCALAR] + specs
    return pl.pallas_call(
        kernel,
        out_shape=outs[0] if single else outs,
        in_specs=specs,
        out_specs=WHOLE if single else (WHOLE,) * len(outs),
        scratch_shapes=list(scratch),
        cost_estimate=pl.CostEstimate(
            flops=costs.get("flops", 1 << 20),
            bytes_accessed=costs.get("moved", 1 << 20),
            transcendentals=costs.get("exps", 0),
        ),
        compiler_params=pltpu.CompilerParams(vmem_limit_bytes=room),
    )(*args)


def split_norm(tp_at, source_rows, gain, weight_rows, tp_count, carried):
    rows, width = source_rows.shape
    half = width // 2
    masks = range(0, tp_count, 2)
    count = len(carried)
    if weight_rows % 128:
        normed = normalize(source_rows, gain)

        def columns(parity):
            return jnp.concatenate(
                [
                    lax.dynamic_slice_in_dim(
                        normed, (tp_at ^ m ^ parity) * weight_rows, weight_rows, 1
                    )
                    for m in masks
                ],
                axis=1,
            )

        return columns(0), columns(1), *carried

    def kernel(at_ref, rows_far, gain_far, *refs):
        far_refs, (own_ref, other_ref), near_refs = refs[:count], refs[count : count + 2], refs[count + 2 : -3]
        rows_ref, gain_ref, done = refs[-3:]
        pairs = [(rows_far, rows_ref), (gain_far, gain_ref), *zip(far_refs, near_refs)]
        copies = [
            pltpu.make_async_copy(source, target, done.at[at])
            for at, (source, target) in enumerate(pairs)
        ]
        for copy in copies:
            copy.start()
        copies[0].wait()
        copies[1].wait()
        widened = rows_ref[...].astype(F32)
        factor = lax.rsqrt(jnp.mean(widened * widened, axis=-1, keepdims=True) + EPSILON)
        for parity, out_ref in ((0, own_ref), (1, other_ref)):
            for place, m in enumerate(masks):
                start = pl.multiple_of((at_ref[0] ^ (m + parity)) * weight_rows, 128)
                at = pl.ds(start, weight_rows)
                piece = rows_ref[:, at].astype(F32) * factor * gain_ref[:, at]
                out_ref[:, place * weight_rows : (place + 1) * weight_rows] = piece.astype(BF16)
        for copy in copies[2:]:
            copy.wait()

    outs = (shape_of((rows, half), BF16), shape_of((rows, half), BF16))
    outs += tuple(shape_of(array.shape, array.dtype) for array in carried)
    return resident(
        kernel,
        outs,
        source_rows,
        gain[None],
        *carried,
        scalar=tp_at,
        far=2 + count,
        scratch=[
            pltpu.VMEM((rows, width), BF16),
            pltpu.VMEM((1, width), F32),
            pltpu.SemaphoreType.DMA((2 + count,)),
        ],
        flops=8 * rows * width,
    )


def project_some(own, other, places, weights):
    rows = own.shape[0]
    weight_rows, kv_width = weights[0][0].shape
    counts = [len(kind) for kind in weights]
    flat = [block for kind in weights for block in kind]

    def kernel(own_ref, other_ref, *refs):
        block_refs, out_refs = refs[: len(flat)], refs[len(flat) :]
        lhs = jnp.concatenate([own_ref[...], other_ref[...]], axis=0)
        for kind, out_ref in enumerate(out_refs):
            start = sum(counts[:kind])
            total = None
            for place, ref in zip(places[kind], block_refs[start : start + counts[kind]]):
                term = dot(lhs[:, place * weight_rows : (place + 1) * weight_rows], ref[...])
                total = term if total is None else total + term
            out_ref[...] = total

    outs = (shape_of((2 * rows, kv_width), F32),) * 2
    flops = 4 * rows * len(flat) * weight_rows * kv_width
    return resident(kernel, outs, own, other, *flat, flops=flops)


def project_rest(own, other, places, early, weights):
    rows = own.shape[0]
    weight_rows, kv_width = weights[0][0].shape
    counts = [len(kind) for kind in weights]
    flat = [block for kind in weights for block in kind]

    def kernel(own_ref, other_ref, *refs):
        early_refs, block_refs, (near_ref, far_ref) = refs[:2], refs[2:-2], refs[-2:]
        lhs = jnp.concatenate([own_ref[...], other_ref[...]], axis=0)
        sums = []
        for kind in range(2):
            total = early_refs[kind][...]
            start = sum(counts[:kind])
            for place, ref in zip(places[kind], block_refs[start : start + counts[kind]]):
                columns = lhs[:, place * weight_rows : (place + 1) * weight_rows]
                total = total + dot(columns, ref[...])
            sums.append(total)
        for head in range(KV_HEADS):
            at = slice(head * HEAD_DIM, (head + 1) * HEAD_DIM)
            packed = jnp.concatenate([sums[0][:, at], sums[1][:, at]], axis=1)
            near_ref[head] = packed[:rows]
            far_ref[head] = packed[rows:]

    outs = (
        shape_of((KV_HEADS, rows, 2 * HEAD_DIM), F32),
        shape_of((KV_HEADS, rows, 2 * HEAD_DIM), F32),
    )
    return resident(
        kernel, outs, own, other, *early, *flat, flops=4 * rows * len(flat) * weight_rows * kv_width
    )


def stack(arrays, lead=()):
    lead = lead or (len(arrays),)

    def kernel(*refs):
        for at, ref in enumerate(refs[:-1]):
            place = (at // lead[1], at % lead[1]) if len(lead) == 2 else (at,)
            refs[-1][place] = ref[...]

    out = shape_of((*lead, *arrays[0].shape), arrays[0].dtype)
    return resident(kernel, out, *arrays, kept=0, loaded=len(arrays))


def add_parts(own, theirs):
    def kernel(own_ref, theirs_ref, out_ref):
        out_ref[...] = (own_ref[...] + theirs_ref[...]).astype(BF16)

    return resident(kernel, shape_of(own.shape, BF16), own, theirs)


def pack_target(target_rows, cotangent, gain):
    def kernel(rows_far, gain_far, cot_far, out_ref, rows_ref, gain_ref, done):
        pairs = ((rows_far, rows_ref), (gain_far, gain_ref), (cot_far, out_ref.at[1]))
        copies = [
            pltpu.make_async_copy(source, target, done.at[at])
            for at, (source, target) in enumerate(pairs)
        ]
        for copy in copies:
            copy.start()
        copies[0].wait()
        copies[1].wait()
        out_ref[0] = normalize(rows_ref[...], gain_ref[...])
        copies[2].wait()

    return resident(
        kernel,
        shape_of((2, *target_rows.shape), BF16),
        target_rows,
        gain[None],
        cotangent,
        far=3,
        scratch=[
            pltpu.VMEM(target_rows.shape, BF16),
            pltpu.VMEM((1, target_rows.shape[1]), F32),
            pltpu.SemaphoreType.DMA((3,)),
        ],
    )


def project_target(pieces, query_weight, out_weight):
    count = sum(piece.shape[1] for piece in pieces)
    heads = query_weight.shape[1] // HEAD_DIM

    def kernel(*refs):
        piece_refs, (query_ref, weight_ref, out_ref) = refs[:-3], refs[-3:]
        rows = jnp.concatenate([ref[0] for ref in piece_refs], axis=0)
        queries = stacked(transposed(dot(rows, query_ref[...]))).astype(BF16)
        out_ref[0:HEAD_DIM, :] = queries * jnp.asarray(SCALE, BF16)
        cot = jnp.concatenate([ref[1] for ref in piece_refs], axis=0)
        out_ref[HEAD_DIM:, :] = stacked(nt_dot(weight_ref[...], cot)).astype(BF16)

    out = shape_of((2 * HEAD_DIM, heads * count), BF16)
    flops = 4 * count * query_weight.size
    return resident(kernel, out, *pieces, query_weight, out_weight, kept=0, flops=flops)


def hold_own(pieces, pair):
    count = sum(piece.shape[1] for piece in pieces)

    def kernel(*refs):
        piece_refs, (pair_ref, near_ref, out_ref) = refs[:-3], refs[-3:]
        near_ref[...] = pair_ref[...]
        out_ref[...] = jnp.concatenate([ref[1] for ref in piece_refs], axis=0)

    outs = (shape_of(pair.shape, BF16), shape_of((count, pieces[0].shape[2]), BF16))
    return resident(kernel, outs, *pieces, pair, kept=1, loaded=len(pieces), fetched=1)


def gather_cotangents(pieces):
    blocks, piece_rows, width = pieces[0].shape
    count = piece_rows * len(pieces)

    def kernel(*refs):
        piece_refs, out_ref = (refs[-2], *refs[:-2]), refs[-1]
        for block in range(blocks):
            rows = jnp.concatenate([ref[block] for ref in piece_refs], axis=0)
            out_ref[block * count : (block + 1) * count, :] = rows

    out = shape_of((blocks * count, width), BF16)
    return resident(kernel, out, *pieces[1:], pieces[0], kept=0, fetched=1)


def forward_all(pairs, kv):
    blocks = len(pairs)
    lanes = pairs[0].shape[1]
    rows = kv.shape[0]
    chunk = chunk_for(rows)

    def kernel(*refs):
        pair_refs, kv_ref = refs[:blocks], refs[blocks]
        out_ref, stat_ref, *score_refs = refs[blocks + 1 :]
        zeros = jnp.zeros((HEAD_DIM, lanes), BF16)
        for block, pair_ref in enumerate(pair_refs):
            query = jnp.concatenate([pair_ref[0:HEAD_DIM, :], zeros], axis=0)
            score_ref = score_refs[block]
            peak = jnp.full((8, lanes), -jnp.inf, F32)
            for start in range(0, rows, chunk):
                scores = dot(kv_ref[start : start + chunk, :], query)
                score_ref[start : start + chunk, :] = scores
                peak = jnp.maximum(peak, jnp.max(scores.reshape(chunk // 8, 8, lanes), axis=0))
            row_max = jnp.max(peak, axis=0, keepdims=True)
            total = jnp.zeros((8, lanes), F32)
            summed = jnp.zeros((HEAD_DIM, lanes), F32)
            for start in range(0, rows, chunk):
                weights = jnp.exp(score_ref[start : start + chunk, :] - row_max)
                total = total + jnp.sum(weights.reshape(chunk // 8, 8, lanes), axis=0)
                values = kv_ref[start : start + chunk, HEAD_DIM:]
                summed = summed + tn_dot(values, weights.astype(BF16))
            total = jnp.sum(total, axis=0, keepdims=True)
            part = summed / total
            out_ref[block] = part
            stat_ref[2 * block : 2 * block + 1, :] = row_max + jnp.log(total)
            stat_ref[2 * block + 1 : 2 * block + 2, :] = jnp.sum(
                pair_ref[HEAD_DIM:, :].astype(F32) * part, axis=0, keepdims=True
            )

    outs = (shape_of((blocks, HEAD_DIM, lanes), F32), shape_of((2 * blocks, lanes), F32))
    outs += (shape_of((rows, lanes), F32),) * blocks
    return resident(
        kernel,
        outs,
        *pairs,
        kv,
        room=ROOM,
        flops=8 * blocks * rows * lanes * HEAD_DIM,
        exps=blocks * rows * lanes,
    )


def combine_stats(stats, parts):
    blocks, _, lanes = parts.shape

    def kernel(*refs):
        stat_refs, part_ref = refs[:blocks], refs[blocks]
        out_ref, *share_refs = refs[blocks + 1 :]
        for block in range(blocks):
            logs, deltas = [], []
            for peer, stat_ref in enumerate(stat_refs):
                at = 2 * (block ^ peer)
                logs.append(stat_ref[at : at + 1, :])
                deltas.append(stat_ref[at + 1 : at + 2, :])
            peak = logs[0]
            for log in logs[1:]:
                peak = jnp.maximum(peak, log)
            shares = [jnp.exp(log - peak) for log in logs]
            total = shares[0]
            delta = shares[0] * deltas[0]
            for share, term in zip(shares[1:], deltas[1:]):
                total = total + share
                delta = delta + share * term
            out_ref[2 * block : 2 * block + 1, :] = peak + jnp.log(total)
            out_ref[2 * block + 1 : 2 * block + 2, :] = delta / total
            share_refs[block][...] = (part_ref[block] * (shares[0] / total)).astype(BF16)

    outs = (shape_of((2 * blocks, lanes), F32),)
    outs += (shape_of((HEAD_DIM, lanes), BF16),) * blocks
    return resident(kernel, outs, *stats, parts, kept=1)


def backward_some(order, pairs, scores, stats, kv, sums, slots):
    count = len(order)
    lanes = pairs[0].shape[1]
    rows = kv.shape[0]
    chunk = chunk_for(rows)
    started = [] if sums is None else [sums]

    def kernel(*refs):
        pair_refs, score_refs = refs[:count], refs[count : 2 * count]
        stat_ref, kv_ref = refs[2 * count : 2 * count + 2]
        start_refs = refs[2 * count + 2 : 2 * count + 2 + len(started)]
        outs = refs[2 * count + 2 + len(started) : -1]
        sum_ref = refs[-1]
        zeros = jnp.zeros((HEAD_DIM, lanes), BF16)
        for place, block in enumerate(order):
            query = jnp.concatenate([pair_refs[place][0:HEAD_DIM, :], zeros], axis=0)
            grad = jnp.concatenate([zeros, pair_refs[place][HEAD_DIM:, :]], axis=0)
            log_total = stat_ref[2 * block : 2 * block + 1, :]
            delta = stat_ref[2 * block + 1 : 2 * block + 2, :]
            d_query = jnp.zeros((HEAD_DIM, lanes), F32)
            for start in range(0, rows, chunk):
                at = slice(start, start + chunk)
                pair = kv_ref[at, :]
                probs = jnp.exp(score_refs[place][at, :] - log_total)
                d_scores = (probs * (dot(pair, grad) - delta)).astype(BF16)
                terms = nt_dot(d_scores, query) + nt_dot(probs.astype(BF16), grad)
                if place:
                    terms = terms + sum_ref[at, :]
                elif started:
                    terms = terms + start_refs[0][at, :]
                sum_ref[at, :] = terms
                d_query = d_query + tn_dot(pair[:, :HEAD_DIM], d_scores)
            outs[1 + place][...] = (d_query * SCALE).astype(BF16)
        outs[0][...] = sum_ref[...].astype(outs[0].dtype).reshape(outs[0].shape)

    if slots:
        sum_shape = shape_of((slots, rows // slots, 2 * HEAD_DIM), BF16)
    else:
        sum_shape = shape_of((rows, 2 * HEAD_DIM), F32)
    outs = resident(
        kernel,
        (sum_shape,) + (shape_of((HEAD_DIM, lanes), BF16),) * count,
        *[pairs[block] for block in order],
        *[scores[block] for block in order],
        stats,
        kv,
        *started,
        kept=0 if slots else 1,
        scratch=[pltpu.VMEM((rows, 2 * HEAD_DIM), F32)],
        flops=20 * count * rows * lanes * HEAD_DIM,
        exps=count * rows * lanes,
    )
    return outs[1:], outs[0]


def query_back(parts, query_weight, heads):
    width = query_weight.shape[0]
    count = parts[0].shape[1] // heads
    half = count // 2

    def kernel(*refs):
        part_refs, (weight_ref, last_ref, own_ref, other_ref) = refs[:-4], refs[-4:]
        total = part_refs[0][...].astype(F32)
        for part_ref in (*part_refs[1:], last_ref):
            total = total + part_ref[...].astype(F32)
        grad = transposed(unstacked(total, heads)).astype(BF16)
        upstream = nt_dot(grad, weight_ref[...])
        own_ref[...] = upstream[:half]
        other_ref[...] = upstream[half:].astype(BF16)

    outs = (shape_of((half, width), F32), shape_of((half, width), BF16))
    flops = 2 * count * query_weight.size
    return resident(kernel, outs, *parts[:-1], query_weight, parts[-1], fetched=1, flops=flops)


def share_rows(own, theirs, count):
    rows, width = own.shape
    piece = rows // count

    def kernel(own_ref, theirs_ref, kept_ref, *out_refs):
        kept_ref[...] = own_ref[:piece, :] + theirs_ref[:piece, :].astype(F32)
        for place, out_ref in enumerate(out_refs):
            at = slice((place + 1) * piece, (place + 2) * piece)
            out_ref[...] = (own_ref[at, :] + theirs_ref[at, :].astype(F32)).astype(BF16)

    outs = (shape_of((piece, width), F32),) + (shape_of((piece, width), BF16),) * (count - 1)
    return resident(kernel, outs, own, theirs, kept=0)


def target_finish(kept, received, target_rows, cotangent, gain):
    def kernel(*refs):
        received_refs, (kept_ref, rows_ref, cot_ref, gain_ref, out_ref) = refs[:-5], refs[-5:]
        total = kept_ref[...]
        for ref in received_refs:
            total = total + ref[...].astype(F32)
        back = norm_back(rows_ref[...], gain_ref[...], total)
        out_ref[...] = cot_ref[...].astype(F32) + back

    out = shape_of(kept.shape, F32)
    args = (*received, kept, target_rows, cotangent, gain[None])
    return resident(kernel, out, *args, kept=0, loaded=len(args) - 4, fetched=4)


def attend_sum(parts):
    def kernel(*refs):
        out_ref = refs[-1]
        total = refs[0][...].astype(F32)
        for ref in refs[1:-1]:
            total = total + ref[...].astype(F32)
        out_ref[...] = total.astype(BF16)

    return resident(
        kernel, shape_of(parts[0].shape, BF16), *parts[1:], parts[0], loaded=len(parts) - 1, fetched=1
    )


def weight_grad(attended, cot_parts, heads):
    blocks = len(attended)
    count, width = cot_parts[0].shape
    half = count // 2
    step = 1024 if width % 1024 == 0 else width

    def kernel(*refs):
        attended_refs, cot_refs, (out_ref, wide_ref) = refs[:blocks], refs[blocks:-2], refs[-2:]

        @pl.when(pl.program_id(0) == 0)
        def _():
            for block, attended_ref in enumerate(attended_refs):
                part = unstacked(attended_ref[...].astype(F32), heads).astype(BF16)
                if not block:
                    wide_ref[:, 0:count] = part
                for core in range(2) if block else ():
                    start = count + (core * (blocks - 1) + block - 1) * half
                    wide_ref[:, start : start + half] = part[:, core * half : (core + 1) * half]

        rows = jnp.concatenate([ref[...] for ref in cot_refs], axis=0)
        out_ref[...] = dot(wide_ref[...], rows)

    specs = [pl.BlockSpec(attended[0].shape, lambda i: (0, 0))] * blocks
    specs += [pl.BlockSpec((part.shape[0], step), lambda i: (0, i)) for part in cot_parts]
    return pl.pallas_call(
        kernel,
        grid=(width // step,),
        in_specs=specs,
        out_specs=pl.BlockSpec((heads * HEAD_DIM, step), lambda i: (0, i)),
        out_shape=shape_of((heads * HEAD_DIM, width), F32),
        scratch_shapes=[pltpu.VMEM((heads * HEAD_DIM, blocks * count), BF16)],
        cost_estimate=pl.CostEstimate(
            flops=2 * heads * HEAD_DIM * blocks * count * width,
            bytes_accessed=2 * blocks * count * width,
            transcendentals=0,
        ),
        compiler_params=pltpu.CompilerParams(vmem_limit_bytes=ROOM),
        name="weight_grad",
    )(*attended, *[pltpu.with_memory_space_constraint(part, pltpu.HBM) for part in cot_parts])


def source_back(tp_at, back, held, others, source_rows, gain):
    rows, width = source_rows.shape
    _, count, weight_rows, _ = held.shape

    def kernel(at_ref, back_ref, held_ref, other_ref, rows_ref, gain_ref, out_ref):
        key_grad = jnp.concatenate([back_ref[h][:, :HEAD_DIM] for h in range(KV_HEADS)], axis=1)
        value_grad = jnp.concatenate([back_ref[h][:, HEAD_DIM:] for h in range(KV_HEADS)], axis=1)
        inner = jnp.zeros((rows, 1), F32)
        square = jnp.zeros((rows, 1), F32)
        for place in range(count):
            for parity in (0, 1):
                from_ref = other_ref if parity else held_ref
                key, value = from_ref[0, place], from_ref[1, place]
                start = pl.multiple_of((at_ref[0] ^ (2 * place + parity)) * weight_rows, 128)
                at = pl.ds(start, weight_rows)
                upstream = nt_dot(key_grad, key) + nt_dot(value_grad, value)
                weighted = upstream * gain_ref[:, at]
                widened = rows_ref[:, at].astype(F32)
                inner = inner + jnp.sum(weighted * widened, axis=-1, keepdims=True)
                square = square + jnp.sum(widened * widened, axis=-1, keepdims=True)
                out_ref[:, at] = weighted
        factor = lax.rsqrt(square / width + EPSILON)
        pull = factor**3 * (inner / width)
        out_ref[...] = factor * out_ref[...] - rows_ref[...].astype(F32) * pull

    return resident(
        kernel,
        shape_of((rows, width), F32),
        back,
        held,
        others,
        source_rows,
        gain[None],
        scalar=tp_at,
        kept=0,
        loaded=3,
        fetched=2,
        flops=4 * rows * width * KV_HEADS * HEAD_DIM,
    )


def source_back_plain(tp_at, back, held, others, source_rows, gain):
    rows, width = source_rows.shape
    _, count, weight_rows, _ = held.shape
    fulls = []
    for kind in range(2):
        full = jnp.zeros((width, KV_HEADS * HEAD_DIM), BF16)
        for place in range(count):
            start = (tp_at ^ (2 * place)) * weight_rows
            full = lax.dynamic_update_slice_in_dim(full, held[kind, place], start, 0)
            start = (tp_at ^ (2 * place + 1)) * weight_rows
            full = lax.dynamic_update_slice_in_dim(full, others[kind, place], start, 0)
        fulls.append(full)
    turned = back.transpose(1, 0, 2)
    key_grad = turned[:, :, :HEAD_DIM].reshape(rows, KV_HEADS * HEAD_DIM)
    value_grad = turned[:, :, HEAD_DIM:].reshape(rows, KV_HEADS * HEAD_DIM)
    total = nt_dot(key_grad, fulls[0]) + nt_dot(value_grad, fulls[1])
    return norm_back(source_rows, gain, total)


def body(
    target_rows,
    source_rows,
    target_gain,
    source_gain,
    query_weight,
    key_weight,
    value_weight,
    out_weight,
    out_cotangent,
):
    tp_count = lax.axis_size("tp")
    sp_count = lax.axis_size("sp")
    tp_at = lax.axis_index("tp").astype(jnp.int32)
    own_source = source_rows.shape[0]
    weight_rows = key_weight.shape[0]
    heads = query_weight.shape[1] // HEAD_DIM
    copies = max(1, tp_count // KV_HEADS)
    chips = tp_count // 2
    chip_bits = [1 << b for b in range(1, tp_count.bit_length() - 1)]
    near, far = chip_bits[: len(chip_bits) // 2], chip_bits[len(chip_bits) // 2 :]
    chip_masks = range(0, tp_count, 2)

    packed_t = pack_target(target_rows, out_cotangent, target_gain)
    own_part, other_part, query_near, out_near = split_norm(
        tp_at, source_rows, source_gain, weight_rows, tp_count, (query_weight, out_weight)
    )

    near_rows = [packed_t if m == 0 else swap(packed_t, "tp", m) for m in chip_masks]
    far_rows = [swap(rows, "tp", 1) for rows in near_rows]
    own_pieces = near_rows + far_rows
    pair = project_target(own_pieces, query_near, out_near)
    pair_near, own_cot = hold_own(own_pieces, pair)
    pairs = [pair if k == 0 else swap(pair, "sp", k) for k in range(sp_count)]

    key_found = doubling(key_weight, "tp", far + near)
    value_found = doubling(value_weight, "tp", near + far)
    key_blocks = [key_found[m] for m in chip_masks]
    value_blocks = [value_found[m] for m in chip_masks]

    other_part = swap(other_part, "tp", 1)
    places = [], []
    rest = [], []
    for place, mask in enumerate(chip_masks):
        for kind, late_bits in enumerate((near, far)):
            group = rest if any(mask & bit for bit in late_bits) else places
            group[kind].append(place)
    soon = [[key_blocks[p] for p in places[0]], [value_blocks[p] for p in places[1]]]
    early = project_some(own_part, other_part, places, soon)
    late = [[key_blocks[p] for p in rest[0]], [value_blocks[p] for p in rest[1]]]
    own_sum, other_sum = project_rest(own_part, other_part, rest, early, late)
    held = stack(key_blocks + value_blocks, (2, chips))
    other_sum = swap(other_sum, "tp", 1)
    packed = add_parts(own_sum, other_sum)
    packed = jnp.repeat(packed, copies, axis=0)
    kv = lax.all_to_all(packed, "tp", split_axis=0, concat_axis=0, tiled=True)
    kv = kv.reshape(tp_count * own_source, 2 * HEAD_DIM)

    cot_z = [swap(out_cotangent, "sp", k) for k in range(1, sp_count)]
    cot_z = stack(cot_z)
    cot_near = [cot_z if m == 0 else swap(cot_z, "tp", m) for m in chip_masks]
    near_cot = gather_cotangents(cot_near)
    cot_all = [own_cot, near_cot, swap(near_cot, "tp", 1)]

    parts, own_stats, *scores = forward_all([pair_near] + pairs[1:], kv)
    stats = [own_stats if k == 0 else swap(own_stats, "sp", k) for k in range(sp_count)]
    stats, *shares = combine_stats(stats, parts)
    order = list(range(sp_count // 2, sp_count)) + list(range(sp_count // 2 - 1, -1, -1))
    found, kv_sums = backward_some(order, pairs, scores, stats, kv, None, tp_count)
    query_parts = [part if k == 0 else swap(part, "sp", k) for k, part in zip(order, found)]

    others = swap(held, "tp", 1)
    back = lax.all_to_all(
        kv_sums,
        "tp",
        split_axis=0,
        concat_axis=0,
        tiled=True,
    )
    if copies > 1:
        back = back.reshape(KV_HEADS, copies, own_source, 2 * HEAD_DIM)
        back = back.astype(F32).sum(1).astype(BF16)
    finish = source_back_plain if weight_rows % 128 else source_back
    source_grad = finish(tp_at, back, held, others, source_rows, source_gain)

    mine, theirs = query_back(query_parts, query_near, heads)
    theirs = swap(theirs, "tp", 1)
    kept, *given = share_rows(mine, theirs, chips)
    received = [swap(piece, "tp", m) for m, piece in zip(list(chip_masks)[1:], given)]
    target_grad = target_finish(kept, received, target_rows, out_cotangent, target_gain)

    attended = shares[:1] + [swap(shares[k], "sp", k) for k in range(1, sp_count)]
    attended = attend_sum(attended)
    attended = [attended if k == 0 else swap(attended, "sp", k) for k in range(sp_count)]
    out_weight_grad = weight_grad(attended, cot_all, heads)
    return (target_grad, source_grad, out_weight_grad)


def solution(mesh):
    return jax.shard_map(
        body,
        mesh=mesh,
        in_specs=(
            P(("sp", "tp"), None),
            P(("sp", "tp"), None),
            P(),
            P(),
            P(None, "tp"),
            P("tp", None),
            P("tp", None),
            P("tp", None),
            P(("sp", "tp"), None),
        ),
        out_specs=(P(("sp", "tp"), None), P(("sp", "tp"), None), P("tp", None)),
        check_vma=False,
    )
```
